32 devices in a mesh: grp: 2 (over y), fs: 4 (over z), tp: 4 (over x, core).
Axes of the slice: x: 2, y: 2, z: 4, core: 2. Of those that a mesh axis runs over, the one named last changes fastest.
Arguments:
- tokens: bfloat16 [2048, 2048], P(('grp', 'fs'), 'tp'), parts along dimension 0, may hold values from -6 to 6
- recurrent_norm_gain: float32 [2048], replicated, may hold values from 0.1 to 1.9
- feedforward_norm_gain: float32 [2048], replicated, may hold values from 0.1 to 1.9
- gate_projection_weight: bfloat16 [2048, 2048], P('fs', 'tp'), may hold values from -0.125 to 0.125
- recurrent_projection_weight: bfloat16 [2048, 2048], P('fs', 'tp'), may hold values from -0.125 to 0.125
- convolution_kernel: bfloat16 [4, 2048], P(None, 'tp'), may hold values from -3 to 3
- decay_gate_matrix: bfloat16 [16, 128, 128], P('tp'), may hold values from -0.5 to 0.5
- input_gate_matrix: bfloat16 [16, 128, 128], P('tp'), may hold values from -0.5 to 0.5
- base_decay_logit: float32 [2048], P('tp'), may hold values from 3 to 9
- extra_log_decay: float32 [2048], P(('grp', 'fs')), parts along dimension 0, may hold values from -0.7 to 0
- output_projection_weight: bfloat16 [2048, 2048], P('tp', 'fs'), may hold values from -0.125 to 0.125
- up_projection_weight: bfloat16 [2048, 8192], P('fs', 'tp'), may hold values from -0.125 to 0.125
- down_projection_weight: bfloat16 [8192, 2048], P('tp', 'fs'), may hold values from -0.0625 to 0.0625
Outputs:
- layer_out: bfloat16 [2048, 2048], P(('grp', 'fs'), 'tp'), parts along dimension 0
The draws below stay inside these ranges and needn't reach their ends.
There are 2 independent parts, one for each index of `grp`. The reference program is written for one: setup_inputs(seed, part) draws one part's arguments, and reference() takes and returns one part's arrays. A program takes and returns all parts, laid end to end along the dimension named above; an argument that names none is the same for every part. Nothing has to cross between parts.
All inputs are finite; a program needn't handle non-finite values.
Results may differ from the reference program's by a relative error of at most 0.018.
Values may be sent and summed in bfloat16 or wider, within the bound.
A program may use at most 64 MiB of HBM per device.

```python
import math
import jax
import jax.numpy as jnp
from jax import lax

D = 2048
FF = 8192
BLOCKS = 16
BLOCK_DIM = 128
CONV = 4
SEQUENCE_TOKENS = 256
WIDTH = 2048
TOKENS = 1024
N_TP = 4


def draw_base_decay_logit(key, part):
    key_pick, key_slow, key_fast = jax.random.split(key, 3)
    share = 0.5
    chosen = jax.random.uniform(key_pick, (WIDTH,), jnp.float32) < share
    slow_rate = jnp.exp(jax.random.uniform(key_slow, (WIDTH,), jnp.float32, math.log(0.3), math.log(1.5))) / (4.0 * SEQUENCE_TOKENS)
    fast_rate = 0.25 / jnp.exp(jax.random.uniform(key_fast, (WIDTH,), jnp.float32, math.log(8.0), math.log(25.0)))
    decay_rate = jnp.where(chosen, fast_rate, slow_rate)
    return (-decay_rate - jnp.log(-jnp.expm1(-decay_rate))).astype(jnp.float32)


def draw_extra_log_decay(key, part):
    key_pick, key_depth = jax.random.split(key)
    picked = jax.random.randint(key_pick, (TOKENS,), 0, SEQUENCE_TOKENS) < 3
    depth = jnp.log(jax.random.uniform(key_depth, (TOKENS,), jnp.float32, 0.5, 0.8))
    return jnp.where(picked, depth, 0.0).astype(jnp.float32)


def block_levels(stream_key, shape, cuts, low, largest):
    gain, own = 1.0, jax.random.fold_in(stream_key, 6)
    for axis_at, shards_of in cuts:
        steps = jnp.exp(jax.random.uniform(jax.random.fold_in(own, axis_at), (shards_of,), jnp.float32, low / len(cuts), largest / len(cuts)))
        gain = gain * jnp.repeat(steps, shape[axis_at] // shards_of).reshape([-1 if axis == axis_at else 1 for axis in range(len(shape))])
    return gain


def noise(rng, shape, spread, bound, pieces=(), dtype=jnp.bfloat16):
    drawn = spread * jax.random.normal(rng, shape, jnp.float32)
    if pieces:
        drawn = drawn * block_levels(rng, shape, pieces, -0.22, 0.18)
    return jnp.clip(drawn, -bound, bound).astype(dtype)


def setup_inputs(seed: int = 0, part: int = 0) -> dict:
    key_list = jax.random.split(jax.random.key(seed), 14)
    part_keys = jax.random.split(jax.random.fold_in(key_list[13], part), 14)
    tokens = noise(part_keys[0], (TOKENS, D), 1.0, 6.0, ((0, 4), (1, 4)))
    recurrent_norm_gain = jnp.clip(1.0 + 0.18 * jax.random.normal(key_list[1], (D,), jnp.float32), 0.1, 1.9)
    feedforward_norm_gain = jnp.clip(1.0 + 0.18 * jax.random.normal(key_list[2], (D,), jnp.float32), 0.1, 1.9)
    gate_projection_weight = noise(key_list[3], (D, WIDTH), D ** -0.5, 0.125, ((0, 4), (1, 4)))
    recurrent_projection_weight = noise(key_list[4], (D, WIDTH), D ** -0.5, 0.125, ((0, 4), (1, 4)))
    convolution_kernel = noise(key_list[5], (CONV, WIDTH), 0.5, 3.0, ((1, 4),))
    decay_gate_matrix = noise(key_list[6], (BLOCKS, BLOCK_DIM, BLOCK_DIM), BLOCK_DIM ** -0.5, 0.5, ((0, 4),))
    input_gate_matrix = noise(key_list[7], (BLOCKS, BLOCK_DIM, BLOCK_DIM), BLOCK_DIM ** -0.5, 0.5, ((0, 4),))
    base_decay_logit = draw_base_decay_logit(jax.random.fold_in(key_list[13], 71), part)
    extra_log_decay = draw_extra_log_decay(jax.random.fold_in(jax.random.fold_in(key_list[13], part), 71), part)
    output_projection_weight = noise(key_list[10], (WIDTH, D), WIDTH ** -0.5, 0.125, ((0, 4), (1, 4)))
    up_projection_weight = noise(key_list[11], (D, FF), D ** -0.5, 0.125, ((0, 4), (1, 4)))
    down_projection_weight = noise(key_list[12], (FF, D), FF ** -0.5, 0.0625, ((0, 4), (1, 4)))
    return dict(tokens=tokens, recurrent_norm_gain=recurrent_norm_gain, feedforward_norm_gain=feedforward_norm_gain, gate_projection_weight=gate_projection_weight, recurrent_projection_weight=recurrent_projection_weight, convolution_kernel=convolution_kernel, decay_gate_matrix=decay_gate_matrix, input_gate_matrix=input_gate_matrix, base_decay_logit=base_decay_logit, extra_log_decay=extra_log_decay, output_projection_weight=output_projection_weight, up_projection_weight=up_projection_weight, down_projection_weight=down_projection_weight)


def rms_rows(values_in, norm_gain):
    values = values_in.astype(jnp.float32)
    inverse = lax.rsqrt(lax.optimization_barrier(jnp.mean(values * values, axis=-1, keepdims=True)) + 1e-06)
    return (values * inverse * norm_gain.astype(jnp.float32)).astype(jnp.bfloat16)

def combine(earlier, later):
    return (earlier[0] * later[0], later[0] * earlier[1] + later[1])

def recurrent_state(recurrent_branch_rows, gate_branch_rows, convolution_kernel, decay_gate_matrix, input_gate_matrix, base_decay_logit, extra_log_decay):
    length = recurrent_branch_rows.shape[0]
    taps = convolution_kernel.shape[0]
    padded = jnp.pad(recurrent_branch_rows.astype(jnp.float32), ((taps - 1, 0), (0, 0)))
    conv_sum = jnp.zeros((length, recurrent_branch_rows.shape[1]), jnp.float32)
    for tap_index in range(taps):
        conv_sum = conv_sum + padded[tap_index:tap_index + length] * convolution_kernel[tap_index].astype(jnp.float32)
    conv_rows = conv_sum.astype(jnp.bfloat16)
    blocks = decay_gate_matrix.shape[0]
    blocked = conv_rows.reshape(length, blocks, -1).astype(jnp.float32)
    recurrence_gate = jax.nn.sigmoid(jnp.einsum('tni,nij->tnj', blocked, decay_gate_matrix.astype(jnp.float32)).reshape(length, -1))
    input_rate = jax.nn.sigmoid(jnp.einsum('tni,nij->tnj', blocked, input_gate_matrix.astype(jnp.float32)).reshape(length, -1))
    decay_log_values = -8.0 * jax.nn.softplus(-base_decay_logit) * recurrence_gate + extra_log_decay[:, None]
    decay = jnp.exp(decay_log_values)
    drive = jnp.sqrt(-jnp.expm1(2.0 * decay_log_values)) * input_rate * conv_rows.astype(jnp.float32)
    _, hidden = lax.associative_scan(combine, (decay, drive), axis=0)
    return (hidden * gate_branch_rows.astype(jnp.float32)).astype(jnp.bfloat16)

def split_sum(left_rows, weight):
    block_width = weight.shape[0] // N_TP
    summed = jnp.zeros((left_rows.shape[0], weight.shape[1]), jnp.float32)
    for block_index in range(N_TP):
        lower = block_index * block_width
        partial_value = jnp.dot(left_rows[:, lower:lower + block_width], weight[lower:lower + block_width], preferred_element_type=jnp.float32).astype(jnp.bfloat16)
        summed = summed + lax.optimization_barrier(partial_value).astype(jnp.float32)
    return summed

def reference(tokens, recurrent_norm_gain, feedforward_norm_gain, gate_projection_weight, recurrent_projection_weight, convolution_kernel, decay_gate_matrix, input_gate_matrix, base_decay_logit, extra_log_decay, output_projection_weight, up_projection_weight, down_projection_weight):
    sequence_count = tokens.shape[0]
    sequence_batch = sequence_count // SEQUENCE_TOKENS
    normed = rms_rows(tokens, recurrent_norm_gain)
    gate_branch_rows = jax.nn.gelu(jnp.dot(normed, gate_projection_weight, preferred_element_type=jnp.float32)).astype(jnp.bfloat16)
    recurrent_branch_rows = jnp.dot(normed, recurrent_projection_weight, preferred_element_type=jnp.float32).astype(jnp.bfloat16)
    mixed_output = jax.vmap(recurrent_state, in_axes=(0, 0, None, None, None, None, 0))(recurrent_branch_rows.reshape(sequence_batch, SEQUENCE_TOKENS, -1), gate_branch_rows.reshape(sequence_batch, SEQUENCE_TOKENS, -1), convolution_kernel, decay_gate_matrix, input_gate_matrix, base_decay_logit, extra_log_decay.reshape(sequence_batch, SEQUENCE_TOKENS)).reshape(sequence_count, -1)
    residual = (tokens.astype(jnp.float32) + split_sum(mixed_output, output_projection_weight)).astype(jnp.bfloat16)
    channel_in = rms_rows(residual, feedforward_norm_gain)
    upward = jnp.maximum(jnp.dot(channel_in, up_projection_weight, preferred_element_type=jnp.float32), 0.0)
    squared = (upward * upward).astype(jnp.bfloat16)
    return (residual.astype(jnp.float32) + split_sum(squared, down_projection_weight)).astype(jnp.bfloat16)
```

```python
import functools

import jax
import jax.numpy as jnp
from jax import lax
from jax.experimental import pallas as pl
from jax.experimental.pallas import tpu as pltpu
from jax.sharding import PartitionSpec as P

MESH = pl.DeviceIdType.MESH


def rms_rows(values_in, norm_gain):
    values = values_in.astype(jnp.float32)
    inverse = lax.rsqrt(jnp.mean(values * values, axis=-1, keepdims=True) + 1e-06)
    return (values * inverse * norm_gain).astype(jnp.bfloat16)


def combine(earlier, later):
    return (earlier[0] * later[0], later[0] * earlier[1] + later[1])


def recurrent_state(
    recurrent_branch_rows,
    gate_branch_rows,
    convolution_kernel,
    decay_gate_matrix,
    input_gate_matrix,
    base_decay_logit,
    extra_log_decay,
):
    length = recurrent_branch_rows.shape[0]
    taps = convolution_kernel.shape[0]
    padded = jnp.pad(recurrent_branch_rows.astype(jnp.float32), ((taps - 1, 0), (0, 0)))
    conv_sum = jnp.zeros((length, recurrent_branch_rows.shape[1]), jnp.float32)
    for tap_index in range(taps):
        conv_sum = conv_sum + padded[tap_index : tap_index + length] * convolution_kernel[
            tap_index
        ].astype(jnp.float32)
    conv_rows = conv_sum.astype(jnp.bfloat16)
    blocks = decay_gate_matrix.shape[0]
    blocked = conv_rows.reshape(length, blocks, -1)
    recurrence_gate = jax.nn.sigmoid(
        jnp.einsum(
            "tni,nij->tnj", blocked, decay_gate_matrix, preferred_element_type=jnp.float32
        ).reshape(length, -1)
    )
    input_rate = jax.nn.sigmoid(
        jnp.einsum(
            "tni,nij->tnj", blocked, input_gate_matrix, preferred_element_type=jnp.float32
        ).reshape(length, -1)
    )
    decay_log_values = (
        -8.0 * jax.nn.softplus(-base_decay_logit) * recurrence_gate + extra_log_decay[:, None]
    )
    decay = jnp.exp(decay_log_values)
    drive = (
        jnp.sqrt(-jnp.expm1(2.0 * decay_log_values)) * input_rate * conv_rows.astype(jnp.float32)
    )
    _, hidden = lax.associative_scan(combine, (decay, drive), axis=0)
    return (hidden * gate_branch_rows.astype(jnp.float32)).astype(jnp.bfloat16)


def per_device(
    tokens,
    recurrent_norm_gain,
    feedforward_norm_gain,
    gate_projection_weight,
    recurrent_projection_weight,
    convolution_kernel,
    decay_gate_matrix,
    input_gate_matrix,
    base_decay_logit,
    extra_log_decay,
    output_projection_weight,
    up_projection_weight,
    down_projection_weight,
):
    whole_rows = lax.all_gather(tokens, "tp", axis=1, tiled=True)
    normed = rms_rows(whole_rows, recurrent_norm_gain)
    columns = normed
    gate_pre = jnp.dot(
        columns,
        lax.all_gather(gate_projection_weight, "fs", axis=0, tiled=True),
        preferred_element_type=jnp.float32,
    )
    recur_pre = jnp.dot(
        columns,
        lax.all_gather(recurrent_projection_weight, "fs", axis=0, tiled=True),
        preferred_element_type=jnp.float32,
    )
    gate_branch_rows = jax.nn.gelu(gate_pre).astype(jnp.bfloat16)
    recurrent_branch_rows = recur_pre.astype(jnp.bfloat16)
    mixed_output = recurrent_state(
        recurrent_branch_rows,
        gate_branch_rows,
        convolution_kernel,
        decay_gate_matrix,
        input_gate_matrix,
        base_decay_logit,
        extra_log_decay,
    )
    partials = jnp.dot(
        mixed_output,
        lax.all_gather(output_projection_weight, "fs", axis=1, tiled=True),
        preferred_element_type=jnp.float32,
    )
    residual = (
        tokens.astype(jnp.float32)
        + lax.psum_scatter(
            partials.astype(jnp.bfloat16), "tp", scatter_dimension=1, tiled=True
        ).astype(jnp.float32)
    ).astype(jnp.bfloat16)
    middle = lax.all_gather(residual, "tp", axis=1, tiled=True)
    channel_in = rms_rows(middle, feedforward_norm_gain)
    columns = channel_in
    upward = jnp.dot(
        columns,
        lax.all_gather(up_projection_weight, "fs", axis=0, tiled=True),
        preferred_element_type=jnp.float32,
    )
    positive = jnp.maximum(upward, 0.0)
    squared = (positive * positive).astype(jnp.bfloat16)
    down_terms = jnp.dot(
        squared,
        lax.all_gather(down_projection_weight, "fs", axis=1, tiled=True),
        preferred_element_type=jnp.float32,
    )
    summed_down = lax.psum_scatter(
        down_terms.astype(jnp.bfloat16), "tp", scatter_dimension=1, tiled=True
    ).astype(jnp.float32)
    return (residual.astype(jnp.float32) + summed_down).astype(jnp.bfloat16)

PIECES = 2
POOL = 157
TILE = 64


class Link:
    def __init__(self, pool):
        self.pool, self.started = pool, []

    def send(self, source, target, arrival, peer, only=None):
        moving = pltpu.make_async_remote_copy(
            src_ref=source,
            dst_ref=target,
            send_sem=self.pool.at[len(self.started)],
            recv_sem=arrival,
            device_id=peer,
            device_id_type=MESH,
        )
        self.started.append((moving, only))
        if only is None:
            moving.start()
        else:
            pl.when(only)(moving.start)

    def finish(self):
        for moving, only in self.started:
            if only is None:
                moving.wait_send()
            else:
                pl.when(only)(moving.wait_send)


def arrive(target, arrival, peer):
    pltpu.make_async_remote_copy(
        src_ref=target,
        dst_ref=target,
        send_sem=arrival,
        recv_sem=arrival,
        device_id=peer,
        device_id_type=MESH,
    ).wait_recv()


class Where:
    def __init__(self):
        self.place, self.row = lax.axis_index("fs"), lax.axis_index("tp")
        self.plane = lax.axis_index("grp")
        place = self.place
        self.near = place + 1 - 2 * lax.rem(place, 2)
        self.mid = 3 - place
        self.inner = lax.rem((place + 1) // 2, 2)
        self.is_inner, self.is_outer = self.inner == 1, self.inner == 0
        far = place // 2
        self.order = [place, self.near, 2 - far, 3 - 3 * far]
        self.across, self.beside, self.corner = self.row ^ 2, self.row ^ 1, self.row ^ 3


def greet(at):
    barrier = pltpu.get_barrier_semaphore()
    peers = [{"fs": spot} for spot in at.order[1:]]
    peers += [{"tp": at.beside}, {"tp": at.across}, {"grp": 1 - at.plane}]
    for peer in peers:
        pl.semaphore_signal(barrier, inc=1, device_id=peer, device_id_type=MESH)
    pl.semaphore_wait(barrier, len(peers))


class Gather:
    def __init__(self, at, link, own, held, arrived):
        self.at, self.link, self.own, self.held, self.arrived = at, link, own, held, arrived
        self.step = own.shape[0] // PIECES

    def piece(self, origin, part, number):
        return self.held.at[origin, part, pl.ds(number * self.step, self.step)]

    def send(self, source, origin, part, number, peer, only=None):
        self.link.send(
            source,
            self.piece(origin, part, number),
            self.arrived.at[origin, part, number],
            peer,
            only,
        )

    def wait(self, origin, part, number):
        arrive(
            self.piece(origin, part, number),
            self.arrived.at[origin, part, number],
            {"tp": self.at.beside},
        )

    def begin(self):
        at = self.at
        for number in range(PIECES):
            source = self.own.at[pl.ds(number * self.step, self.step)]
            self.send(source, at.place, at.row, number, {"fs": at.near})
            self.send(source, at.place, at.row, number, {"fs": at.mid}, at.is_inner)
            self.send(source, at.place, at.row, number, {"tp": at.across})
            self.send(source, at.place, at.row, number, {"tp": at.beside})

    def relay(self, k):
        at, origin = self.at, self.at.order[k]
        for number in range(PIECES):
            self.wait(origin, at.row, number)
            source = self.piece(origin, at.row, number)
            onward = {"fs": at.mid if k == 1 else at.near}
            self.send(source, origin, at.row, number, onward, at.is_inner)
            self.send(source, origin, at.row, number, {"tp": at.across})
            self.send(source, origin, at.row, number, {"tp": at.beside})

    def cross(self, k):
        at, origin = self.at, self.at.order[k]
        for number in range(PIECES):
            self.wait(origin, at.across, number)
            source = self.piece(origin, at.across, number)
            self.send(source, origin, at.across, number, {"tp": at.beside})

    def normalise(self, k, norm_gain, target):
        at, origin = self.at, self.at.order[k]
        for number in range(PIECES):
            self.wait(origin, at.beside, number)
            self.wait(origin, at.corner, number)
        length, width = self.own.shape
        parts_of = self.held.shape[1]

        def tile(index, carry):
            rows = pl.ds(pl.multiple_of(index * TILE, TILE), TILE)
            parts = [self.held[origin, p, rows].astype(jnp.float32) for p in range(parts_of)]
            total = sum(jnp.sum(part * part, axis=-1, keepdims=True) for part in parts)
            inverse = lax.rsqrt(total / (parts_of * width) + 1e-06)
            for number, part in enumerate(parts):
                columns = pl.ds(number * width, width)
                target[rows, columns] = (part * inverse * norm_gain[:, columns]).astype(
                    target.dtype
                )
            return carry

        lax.fori_loop(0, length // TILE, tile, 0)


class Scatter:
    def __init__(self, at, link, terms, from_core, to_x, from_x, to_z, from_z, sems):
        self.at, self.link, self.terms = at, link, terms
        self.from_core, self.to_x, self.from_x = from_core, to_x, from_x
        self.to_z, self.from_z = to_z, from_z
        self.core_sems, self.x_sems, self.z_sems = sems
        self.step = terms.shape[2] // PIECES

    def rows(self, number):
        return pl.ds(number * self.step, self.step)

    def core(self, k):
        at = self.at
        for side, part in ((1, at.corner), (0, at.beside)):
            self.link.send(
                self.terms.at[k, part],
                self.from_core.at[side, k],
                self.core_sems.at[side, k],
                {"tp": at.beside},
            )

    def x(self, k):
        at = self.at
        arrive(self.from_core.at[1, k], self.core_sems.at[1, k], {"tp": at.beside})
        for number in range(PIECES):
            rows = self.rows(number)
            mine = self.terms[k, at.across, rows].astype(jnp.float32)
            theirs = self.from_core[1, k, rows].astype(jnp.float32)
            self.to_x[k, rows] = (mine + theirs).astype(self.to_x.dtype)
            self.link.send(
                self.to_x.at[k, rows],
                self.from_x.at[k, rows],
                self.x_sems.at[k, number],
                {"tp": at.across},
            )

    def joined(self, k, number):
        rows = self.rows(number)
        mine = self.terms[k, self.at.row, rows].astype(jnp.float32)
        mine = mine + self.from_core[0, k, rows].astype(jnp.float32)
        return mine + self.from_x[k, rows].astype(jnp.float32)

    def taken(self, slot, number):
        rows = self.rows(number)
        arrive(
            self.from_z.at[slot, rows], self.z_sems.at[slot, number], {"fs": self.at.near}
        )
        return self.from_z[slot, rows].astype(jnp.float32)

    def ready(self, k, number):
        at, rows = self.at, self.rows(number)
        if not number:
            arrive(self.from_core.at[0, k], self.core_sems.at[0, k], {"tp": at.beside})
        arrive(self.from_x.at[k, rows], self.x_sems.at[k, number], {"tp": at.across})

    def z(self, k):
        at = self.at
        comes = {2: 0, 3: 1, 1: 4}[k]
        peer = at.near if k == 1 else at.near + at.inner * (at.mid - at.near)
        slot = {2: 3 * at.inner, 3: 1 + 3 * at.inner, 1: 2}[k]
        for number in range(PIECES):
            rows = self.rows(number)
            self.ready(k, number)

            @pl.when(at.is_inner)
            def _():
                total = self.joined(k, number) + self.taken(comes, number)
                self.to_z[k, rows] = total.astype(self.to_z.dtype)

            @pl.when(at.is_outer)
            def _():
                self.to_z[k, rows] = self.joined(k, number).astype(self.to_z.dtype)

            self.link.send(
                self.to_z.at[k, rows],
                self.from_z.at[slot, rows],
                self.z_sems.at[slot, number],
                {"fs": peer},
            )

    def own(self, base, target):
        at = self.at
        for number in range(PIECES):
            rows = self.rows(number)
            self.ready(0, number)

            @pl.when(at.is_inner)
            def _():
                total = self.joined(0, number) + self.taken(2, number) + self.taken(3, number)
                target[rows] = (base[rows].astype(jnp.float32) + total).astype(target.dtype)

            @pl.when(at.is_outer)
            def _():
                total = self.joined(0, number) + self.taken(2, number)
                target[rows] = (base[rows].astype(jnp.float32) + total).astype(target.dtype)


class Weights:
    def __init__(self, at, link, chunks, moves):
        self.at, self.link, self.chunks, self.moves = at, link, chunks, moves

    def spread(self, number, k):
        at, (leaving, landing) = self.at, self.chunks[number]
        owner = at.order[k]
        self.link.send(
            leaving(owner, at.plane),
            landing(at.place, at.plane),
            self.moves.at[number, 0, at.place],
            {"fs": owner},
        )

    def forward(self, number, k):
        at, (_, landing) = self.at, self.chunks[number]
        source, peer = at.order[k], {"grp": 1 - at.plane}
        here = landing(source, at.plane)
        arrive(here, self.moves.at[number, 0, source], peer)
        self.link.send(here, here, self.moves.at[number, 1, source], peer)

    def wait(self, number):
        at, (_, landing) = self.at, self.chunks[number]
        for source in at.order[1:]:
            arrive(
                landing(source, 1 - at.plane),
                self.moves.at[number, 1, source],
                {"grp": 1 - at.plane},
            )


def recurrence(both, taps, decay_map, input_map, rate, extra):
    wide = jnp.float32
    size = both.shape[1] // 2
    recur = both[:, size:].astype(jnp.bfloat16).astype(wide)
    length = recur.shape[0]
    position = lax.broadcasted_iota(jnp.int32, recur.shape, 0)
    count = taps.shape[0]
    conv = recur * taps[count - 1 : count].astype(wide)
    for tap in range(count - 1):
        back = count - 1 - tap
        earlier = jnp.where(position >= back, pltpu.roll(recur, back, 0), 0.0)
        conv = conv + earlier * taps[tap : tap + 1].astype(wide)
    conv_rows = conv.astype(jnp.bfloat16)
    recur_gate = jax.nn.sigmoid(jnp.dot(conv_rows, decay_map, preferred_element_type=wide))
    input_rate = jax.nn.sigmoid(jnp.dot(conv_rows, input_map, preferred_element_type=wide))
    log_decay = rate * recur_gate + extra
    decay = jnp.exp(log_decay)
    spread = -jnp.tanh(log_decay) * (decay * decay + 1.0)
    drive = jnp.sqrt(spread) * input_rate * conv_rows.astype(wide)
    back = 1
    while back < length:
        inside = position >= back
        drive = drive + decay * jnp.where(inside, pltpu.roll(drive, back, 0), 0.0)
        if back * 2 < length:
            decay = decay * jnp.where(inside, pltpu.roll(decay, back, 0), 1.0)
        back *= 2
    gate_rows = jax.nn.gelu(both[:, :size]).astype(jnp.bfloat16)
    return (drive * gate_rows.astype(wide)).astype(jnp.bfloat16)


def layer_kernel(
    tokens, gain_one, gain_two, taps, decay_map, input_map, logit, extra_own,
    gate, recur, outward, upward, downward, out,
    held_one, held_two, residual, normed, both_w, out_w, up_w, down_w, extra,
    terms, from_core, to_x, from_x, to_z, from_z,
    pool, arrived, core_sems, x_sems, z_sems, moves, extra_sems, local_sems,
):
    at = Where()
    greet(at)
    link = Link(pool)
    length, width = tokens.shape
    depth, size = gate.shape[0], taps.shape[1] // 4
    hidden = up_w.shape[1]
    half, place = depth // 2, at.place

    def spot(start, count, step):
        return pl.ds(pl.multiple_of(start, step), count)

    def by_rows(weight, joined, columns, first, pieces, piece):
        share = half // pieces

        def leaving(owner, plane):
            rows = spot(plane * half + piece * share, share, share)
            return weight.at[rows, spot(owner * columns, columns, columns)]

        def landing(source, plane):
            rows = spot(source * depth + plane * half + piece * share, share, share)
            return joined.at[rows, pl.ds(first, columns)]

        return leaving, landing

    def by_columns(weight, joined, rows_of, pieces, piece):
        share = rows_of // 2 // pieces

        def leaving(owner, plane):
            return weight.at[
                spot(owner * rows_of + plane * rows_of // 2 + piece * share, share, share)
            ]

        def landing(source, plane):
            rows = spot(plane * rows_of // 2 + piece * share, share, share)
            return joined.at[rows, spot(source * width, width, width)]

        return leaving, landing

    chunks = [
        by_rows(gate, both_w, size, 0, 1, 0),
        by_rows(recur, both_w, size, size, 1, 0),
        by_columns(outward, out_w, size, 1, 0),
        by_rows(upward, up_w, hidden, 0, 2, 0),
        by_rows(upward, up_w, hidden, 0, 2, 1),
        by_columns(downward, down_w, hidden, 2, 0),
        by_columns(downward, down_w, hidden, 2, 1),
    ]
    weights = Weights(at, link, chunks, moves)

    def spread(numbers, ks=(1, 2, 3)):
        for k in ks:
            for number in numbers:
                weights.spread(number, k)

    def forward(numbers, ks=(1, 2, 3)):
        for k in ks:
            for number in numbers:
                weights.forward(number, k)

    first = Gather(at, link, tokens, held_one, arrived.at[0])
    first.begin()
    spread((0, 1), (1,))
    for k in range(1, 4):
        link.send(
            extra_own.at[0], extra.at[place], extra_sems.at[place], {"fs": at.order[k]}
        )
    extra[place] = extra_own[0]
    local = []
    for number, (leaving, landing) in enumerate(chunks):
        for plane in range(2):
            moving = pltpu.make_async_copy(
                leaving(place, plane), landing(place, plane), local_sems.at[number, plane]
            )
            moving.start()
            local.append(moving)
    held_one[place, at.row] = tokens[...]
    first.relay(1)
    spread((0, 1), (2, 3))
    first.cross(0)
    first.relay(2)
    first.cross(1)
    forward((0, 1), (1,))
    first.relay(3)
    spread((2,))
    first.cross(2)
    spread((3,))
    for k in range(3):
        first.normalise(k, gain_one, normed.at[k])
    forward((0, 1), (2, 3))
    for source in at.order[1:]:
        arrive(extra.at[source], extra_sems.at[source], {"fs": at.near})
    first.cross(3)
    forward((2,))
    for moving in local:
        moving.wait()
    for number in range(3):
        weights.wait(number)

    own_taps = taps[:, spot(place * size, size, size)]
    own_logit = logit[:, spot(place * size, size, size)]
    rate = -8.0 * (
        jnp.maximum(-own_logit, 0.0) + jnp.log1p(jnp.exp(-jnp.abs(own_logit)))
    )

    def mix(k):
        both = jnp.dot(normed[k], both_w[...], preferred_element_type=jnp.float32)
        added = jnp.transpose(jnp.broadcast_to(extra[at.order[k]], (size, length)))
        mixed = recurrence(both, own_taps, decay_map[place], input_map[place], rate, added)
        for part in range(4):
            terms[0, k, part] = jnp.dot(
                mixed, out_w[:, pl.ds(part * width, width)], preferred_element_type=jnp.float32
            ).astype(terms.dtype)

    def scatter(turn):
        return Scatter(
            at, link, terms.at[turn], from_core.at[turn], to_x.at[turn], from_x.at[turn],
            to_z.at[turn], from_z.at[turn],
            (core_sems.at[turn], x_sems.at[turn], z_sems.at[turn]),
        )

    summed = scatter(0)
    mix(2)
    summed.core(2)
    first.normalise(3, gain_one, normed.at[3])
    mix(3)
    summed.core(3)
    summed.x(2)
    mix(1)
    summed.core(1)
    summed.x(3)
    mix(0)
    summed.core(0)
    summed.x(1)
    summed.z(2)
    spread((4,), (1,))
    summed.x(0)
    summed.z(3)
    spread((4,), (2, 3))
    forward((3,))
    summed.z(1)
    spread((5,), (1,))
    summed.own(tokens, residual)

    second = Gather(at, link, residual, held_two, arrived.at[1])
    second.begin()
    spread((5,), (2, 3))
    held_two[place, at.row] = residual[...]
    second.relay(1)
    spread((6,), (1,))
    second.cross(0)
    second.relay(2)
    forward((4,))
    second.cross(1)
    second.relay(3)
    spread((6,), (2, 3))
    second.cross(2)
    for k in range(3):
        second.normalise(k, gain_two, normed.at[k])
    forward((5,))
    second.cross(3)
    for number in (3, 4):
        weights.wait(number)
    forward((6,))
    for number in (5, 6):
        weights.wait(number)

    def feed(k):
        raised = jnp.dot(normed[k], up_w[...], preferred_element_type=jnp.float32)
        positive = jnp.maximum(raised, 0.0)
        squared = (positive * positive).astype(jnp.bfloat16)
        for part in range(4):
            terms[1, k, part] = jnp.dot(
                squared, down_w[:, pl.ds(part * width, width)], preferred_element_type=jnp.float32
            ).astype(terms.dtype)

    last = scatter(1)
    feed(2)
    last.core(2)
    second.normalise(3, gain_two, normed.at[3])
    feed(3)
    last.core(3)
    last.x(2)
    feed(1)
    last.core(1)
    last.x(3)
    feed(0)
    last.core(0)
    last.x(1)
    last.z(2)
    last.x(0)
    last.z(3)
    last.z(1)
    last.own(residual, out)
    link.finish()


def per_device_owned(
    tokens,
    recurrent_norm_gain,
    feedforward_norm_gain,
    gate_projection_weight,
    recurrent_projection_weight,
    convolution_kernel,
    decay_gate_matrix,
    input_gate_matrix,
    base_decay_logit,
    extra_log_decay,
    output_projection_weight,
    up_projection_weight,
    down_projection_weight,
):
    length, width = tokens.shape
    depth, size = gate_projection_weight.shape[0], gate_projection_weight.shape[1] // 4
    hidden = up_projection_weight.shape[1] // 4
    kind, wide = tokens.dtype, jnp.float32
    vmem, anywhere = pl.BlockSpec(memory_space=pltpu.VMEM), pl.BlockSpec(memory_space=pltpu.HBM)
    dma, block = pltpu.SemaphoreType.DMA, (length, width)
    scratch = [
        ((4, 4) + block, kind),
        ((4, 4) + block, kind),
        (block, kind),
        ((4, length, 4 * width), kind),
        ((4 * depth, 2 * size), kind),
        ((size, 4 * width), kind),
        ((4 * depth, hidden), kind),
        ((hidden, 4 * width), kind),
        ((4, 1, length), wide),
        ((2, 4, 4) + block, kind),
        ((2, 2, 4) + block, kind),
        ((2, 4) + block, kind),
        ((2, 4) + block, kind),
        ((2, 4) + block, kind),
        ((2, 5) + block, kind),
    ]
    return pl.pallas_call(
        layer_kernel,
        out_shape=jax.ShapeDtypeStruct(block, kind),
        in_specs=[vmem] * 8 + [anywhere] * 5,
        out_specs=vmem,
        scratch_shapes=[pltpu.VMEM(*entry) for entry in scratch]
        + [
            dma((POOL,)),
            dma((2, 4, 4, PIECES)),
            dma((2, 2, 4)),
            dma((2, 4, PIECES)),
            dma((2, 5, PIECES)),
            dma((7, 2, 4)),
            dma((4,)),
            dma((7, 2)),
        ],
        compiler_params=pltpu.CompilerParams(
            collective_id=1, has_side_effects=True, vmem_limit_bytes=58 * 2**20
        ),
    )(
        tokens,
        recurrent_norm_gain.reshape(1, -1),
        feedforward_norm_gain.reshape(1, -1),
        convolution_kernel,
        decay_gate_matrix,
        input_gate_matrix,
        base_decay_logit.reshape(1, -1),
        extra_log_decay.reshape(1, 1, -1),
        gate_projection_weight,
        recurrent_projection_weight,
        output_projection_weight,
        up_projection_weight,
        down_projection_weight,
    )


def solution(mesh):
    placed = (
        P(("grp", "fs"), "tp"),
        P(),
        P(),
        P("fs", "tp"),
        P("fs", "tp"),
        P(None, "tp"),
        P("tp", None, None),
        P("tp", None, None),
        P("tp"),
        P(("grp", "fs")),
        P("tp", "fs"),
        P("fs", "tp"),
        P("tp", "fs"),
    )
    owners = mesh.shape["fs"] * mesh.shape["tp"]
    fitting = mesh.shape["tp"] == 4 and mesh.shape["grp"] == 2 and mesh.shape["fs"] == 4

    def run(*arrays):
        owned = fitting and arrays[6].shape[0] == owners
        body = per_device_owned if owned else per_device
        return jax.shard_map(
            body, mesh=mesh, in_specs=placed, out_specs=P(("grp", "fs"), "tp"), check_vma=False
        )(*arrays)

    return run
```

```python
import functools

import jax
import jax.numpy as jnp
from jax import lax
from jax.experimental import pallas as pl
from jax.experimental.pallas import tpu as pltpu
from jax.sharding import PartitionSpec as P

MESH = pl.DeviceIdType.MESH


def rms_rows(values_in, norm_gain):
    values = values_in.astype(jnp.float32)
    inverse = lax.rsqrt(jnp.mean(values * values, axis=-1, keepdims=True) + 1e-06)
    return (values * inverse * norm_gain).astype(jnp.bfloat16)


def combine(earlier, later):
    return (earlier[0] * later[0], later[0] * earlier[1] + later[1])


def recurrent_state(
    recurrent_branch_rows,
    gate_branch_rows,
    convolution_kernel,
    decay_gate_matrix,
    input_gate_matrix,
    base_decay_logit,
    extra_log_decay,
):
    length = recurrent_branch_rows.shape[0]
    taps = convolution_kernel.shape[0]
    padded = jnp.pad(recurrent_branch_rows.astype(jnp.float32), ((taps - 1, 0), (0, 0)))
    conv_sum = jnp.zeros((length, recurrent_branch_rows.shape[1]), jnp.float32)
    for tap_index in range(taps):
        conv_sum = conv_sum + padded[tap_index : tap_index + length] * convolution_kernel[
            tap_index
        ].astype(jnp.float32)
    conv_rows = conv_sum.astype(jnp.bfloat16)
    blocks = decay_gate_matrix.shape[0]
    blocked = conv_rows.reshape(length, blocks, -1)
    recurrence_gate = jax.nn.sigmoid(
        jnp.einsum(
            "tni,nij->tnj", blocked, decay_gate_matrix, preferred_element_type=jnp.float32
        ).reshape(length, -1)
    )
    input_rate = jax.nn.sigmoid(
        jnp.einsum(
            "tni,nij->tnj", blocked, input_gate_matrix, preferred_element_type=jnp.float32
        ).reshape(length, -1)
    )
    decay_log_values = (
        -8.0 * jax.nn.softplus(-base_decay_logit) * recurrence_gate + extra_log_decay[:, None]
    )
    decay = jnp.exp(decay_log_values)
    drive = (
        jnp.sqrt(-jnp.expm1(2.0 * decay_log_values)) * input_rate * conv_rows.astype(jnp.float32)
    )
    _, hidden = lax.associative_scan(combine, (decay, drive), axis=0)
    return (hidden * gate_branch_rows.astype(jnp.float32)).astype(jnp.bfloat16)


def per_device(
    tokens,
    recurrent_norm_gain,
    feedforward_norm_gain,
    gate_projection_weight,
    recurrent_projection_weight,
    convolution_kernel,
    decay_gate_matrix,
    input_gate_matrix,
    base_decay_logit,
    extra_log_decay,
    output_projection_weight,
    up_projection_weight,
    down_projection_weight,
):
    whole_rows = lax.all_gather(tokens, "tp", axis=1, tiled=True)
    normed = rms_rows(whole_rows, recurrent_norm_gain)
    columns = normed
    gate_pre = jnp.dot(
        columns,
        lax.all_gather(gate_projection_weight, "fs", axis=0, tiled=True),
        preferred_element_type=jnp.float32,
    )
    recur_pre = jnp.dot(
        columns,
        lax.all_gather(recurrent_projection_weight, "fs", axis=0, tiled=True),
        preferred_element_type=jnp.float32,
    )
    gate_branch_rows = jax.nn.gelu(gate_pre).astype(jnp.bfloat16)
    recurrent_branch_rows = recur_pre.astype(jnp.bfloat16)
    mixed_output = recurrent_state(
        recurrent_branch_rows,
        gate_branch_rows,
        convolution_kernel,
        decay_gate_matrix,
        input_gate_matrix,
        base_decay_logit,
        extra_log_decay,
    )
    partials = jnp.dot(
        mixed_output,
        lax.all_gather(output_projection_weight, "fs", axis=1, tiled=True),
        preferred_element_type=jnp.float32,
    )
    residual = (
        tokens.astype(jnp.float32)
        + lax.psum_scatter(
            partials.astype(jnp.bfloat16), "tp", scatter_dimension=1, tiled=True
        ).astype(jnp.float32)
    ).astype(jnp.bfloat16)
    middle = lax.all_gather(residual, "tp", axis=1, tiled=True)
    channel_in = rms_rows(middle, feedforward_norm_gain)
    columns = channel_in
    upward = jnp.dot(
        columns,
        lax.all_gather(up_projection_weight, "fs", axis=0, tiled=True),
        preferred_element_type=jnp.float32,
    )
    positive = jnp.maximum(upward, 0.0)
    squared = (positive * positive).astype(jnp.bfloat16)
    down_terms = jnp.dot(
        squared,
        lax.all_gather(down_projection_weight, "fs", axis=1, tiled=True),
        preferred_element_type=jnp.float32,
    )
    summed_down = lax.psum_scatter(
        down_terms.astype(jnp.bfloat16), "tp", scatter_dimension=1, tiled=True
    ).astype(jnp.float32)
    return (residual.astype(jnp.float32) + summed_down).astype(jnp.bfloat16)

PIECES = 2
POOL = 125
UP, DOWN = (3, 4), (5, 6)
LIMIT = 58 * 2**20
TILE = 64


class Link:
    def __init__(self, pool):
        self.pool, self.started = pool, []

    def send(self, source, target, arrival, peer, only=None):
        moving = pltpu.make_async_remote_copy(
            src_ref=source,
            dst_ref=target,
            send_sem=self.pool.at[len(self.started)],
            recv_sem=arrival,
            device_id=peer,
            device_id_type=MESH,
        )
        self.started.append((moving, only))
        if only is None:
            moving.start()
        else:
            pl.when(only)(moving.start)

    def finish(self):
        for moving, only in self.started:
            if only is None:
                moving.wait_send()
            else:
                pl.when(only)(moving.wait_send)


def arrive(target, arrival, peer):
    pltpu.make_async_remote_copy(
        src_ref=target,
        dst_ref=target,
        send_sem=arrival,
        recv_sem=arrival,
        device_id=peer,
        device_id_type=MESH,
    ).wait_recv()


class Where:
    def __init__(self):
        self.place, self.row = lax.axis_index("fs"), lax.axis_index("tp")
        self.plane = lax.axis_index("grp")
        place = self.place
        self.near = place + 1 - 2 * lax.rem(place, 2)
        self.mid = 3 - place
        self.inner = lax.rem((place + 1) // 2, 2)
        self.is_inner, self.is_outer = self.inner == 1, self.inner == 0
        far = place // 2
        self.order = [place, self.near, 2 - far, 3 - 3 * far]
        near, other = self.near, self.order[2]
        self.sooner = [place, near + self.inner * (other - near)]
        self.sooner += [other + self.inner * (near - other), self.order[3]]
        self.across, self.beside, self.corner = self.row ^ 2, self.row ^ 1, self.row ^ 3


def greet(at):
    barrier = pltpu.get_barrier_semaphore()
    peers = [{"fs": spot} for spot in at.order[1:]]
    peers += [{"tp": at.beside}, {"tp": at.across}, {"grp": 1 - at.plane}]
    for peer in peers:
        pl.semaphore_signal(barrier, inc=1, device_id=peer, device_id_type=MESH)
    pl.semaphore_wait(barrier, len(peers))


class Gather:
    def __init__(self, at, link, pair, own, held, arrived):
        self.at, self.link, self.own, self.held, self.arrived = at, link, own, held, arrived
        self.pair = pair
        self.step = own.shape[0] // PIECES

    def piece(self, origin, part, number):
        return self.held.at[origin, part, pl.ds(number * self.step, self.step)]

    def send(self, source, origin, part, number, peer, only=None):
        self.link.send(
            source,
            self.piece(origin, part, number),
            self.arrived.at[origin, part, number],
            peer,
            only,
        )

    def wait(self, origin, part, number):
        arrive(
            self.piece(origin, part, number),
            self.arrived.at[origin, part, number],
            {"tp": self.at.beside},
        )

    def begin(self, along=True, aside=True):
        at = self.at
        for number in range(PIECES):
            source = self.own.at[pl.ds(number * self.step, self.step)]
            if along:
                self.send(source, at.place, at.row, number, {"fs": at.near})
                if not self.pair:
                    self.send(source, at.place, at.row, number, {"fs": at.mid}, at.is_inner)
            if aside:
                self.send(source, at.place, at.row, number, {"tp": at.across})
                self.send(source, at.place, at.row, number, {"tp": at.beside})

    def relay(self, k):
        at, origin = self.at, self.at.order[k]
        for number in range(PIECES):
            self.wait(origin, at.row, number)
            source = self.piece(origin, at.row, number)
            onward = {"fs": at.mid if k == 1 else at.near}
            if not self.pair:
                self.send(source, origin, at.row, number, onward, at.is_inner)
            self.send(source, origin, at.row, number, {"tp": at.across})
            self.send(source, origin, at.row, number, {"tp": at.beside})

    def cross(self, k):
        at, origin = self.at, self.at.order[k]
        for number in range(PIECES):
            self.wait(origin, at.across, number)
            source = self.piece(origin, at.across, number)
            self.send(source, origin, at.across, number, {"tp": at.beside})

    def normalise(self, k, norm_gain, target):
        at, origin = self.at, self.at.order[k]
        for number in range(PIECES):
            self.wait(origin, at.beside, number)
            self.wait(origin, at.corner, number)
        length, width = self.own.shape
        parts_of = self.held.shape[1]

        def tile(index, carry):
            rows = pl.ds(pl.multiple_of(index * TILE, TILE), TILE)
            parts = [self.held[origin, p, rows].astype(jnp.float32) for p in range(parts_of)]
            total = sum(jnp.sum(part * part, axis=-1, keepdims=True) for part in parts)
            inverse = lax.rsqrt(total / (parts_of * width) + 1e-06)
            for number, part in enumerate(parts):
                columns = pl.ds(number * width, width)
                target[rows, columns] = (part * inverse * norm_gain[:, columns]).astype(
                    target.dtype
                )
            return carry

        lax.fori_loop(0, length // TILE, tile, 0)


class Scatter:
    def __init__(self, at, link, pair, terms, from_core, to_x, from_x, to_z, from_z, sems):
        self.pair = pair
        self.at, self.link, self.terms = at, link, terms
        self.from_core, self.to_x, self.from_x = from_core, to_x, from_x
        self.to_z, self.from_z = to_z, from_z
        self.core_sems, self.x_sems, self.z_sems = sems
        self.step = terms.shape[2] // PIECES

    def rows(self, number):
        return pl.ds(number * self.step, self.step)

    def core(self, k):
        at = self.at
        for side, part in ((1, at.corner), (0, at.beside)):
            self.link.send(
                self.terms.at[k, part],
                self.from_core.at[side, k],
                self.core_sems.at[side, k],
                {"tp": at.beside},
            )

    def x(self, k):
        at = self.at
        arrive(self.from_core.at[1, k], self.core_sems.at[1, k], {"tp": at.beside})
        for number in range(PIECES):
            rows = self.rows(number)
            mine = self.terms[k, at.across, rows].astype(jnp.float32)
            theirs = self.from_core[1, k, rows].astype(jnp.float32)
            self.to_x[k, rows] = (mine + theirs).astype(self.to_x.dtype)
            self.link.send(
                self.to_x.at[k, rows],
                self.from_x.at[k, rows],
                self.x_sems.at[k, number],
                {"tp": at.across},
            )

    def joined(self, k, number):
        rows = self.rows(number)
        mine = self.terms[k, self.at.row, rows].astype(jnp.float32)
        mine = mine + self.from_core[0, k, rows].astype(jnp.float32)
        return mine + self.from_x[k, rows].astype(jnp.float32)

    def taken(self, slot, number):
        rows = self.rows(number)
        arrive(
            self.from_z.at[slot, rows], self.z_sems.at[slot, number], {"fs": self.at.near}
        )
        return self.from_z[slot, rows].astype(jnp.float32)

    def ready(self, k, number):
        at, rows = self.at, self.rows(number)
        if not number:
            arrive(self.from_core.at[0, k], self.core_sems.at[0, k], {"tp": at.beside})
        arrive(self.from_x.at[k, rows], self.x_sems.at[k, number], {"tp": at.across})

    def z(self, k):
        at = self.at
        comes = {2: 0, 3: 1, 1: 4}[k]
        if self.pair:
            for number in range(PIECES):
                rows = self.rows(number)
                self.ready(k, number)
                self.to_z[k, rows] = self.joined(k, number).astype(self.to_z.dtype)
                self.link.send(
                    self.to_z.at[k, rows],
                    self.from_z.at[2, rows],
                    self.z_sems.at[2, number],
                    {"fs": at.near},
                )
            return
        peer = at.near if k == 1 else at.near + at.inner * (at.mid - at.near)
        slot = {2: 3 * at.inner, 3: 1 + 3 * at.inner, 1: 2}[k]
        for number in range(PIECES):
            rows = self.rows(number)
            self.ready(k, number)

            @pl.when(at.is_inner)
            def _():
                total = self.joined(k, number) + self.taken(comes, number)
                self.to_z[k, rows] = total.astype(self.to_z.dtype)

            @pl.when(at.is_outer)
            def _():
                self.to_z[k, rows] = self.joined(k, number).astype(self.to_z.dtype)

            self.link.send(
                self.to_z.at[k, rows],
                self.from_z.at[slot, rows],
                self.z_sems.at[slot, number],
                {"fs": peer},
            )

    def own(self, base, target):
        at = self.at
        for number in range(PIECES):
            rows = self.rows(number)
            self.ready(0, number)
            if self.pair:
                total = self.joined(0, number) + self.taken(2, number)
                target[rows] = (base[rows].astype(jnp.float32) + total).astype(target.dtype)
                continue

            @pl.when(at.is_inner)
            def _():
                total = self.joined(0, number) + self.taken(2, number) + self.taken(3, number)
                target[rows] = (base[rows].astype(jnp.float32) + total).astype(target.dtype)

            @pl.when(at.is_outer)
            def _():
                total = self.joined(0, number) + self.taken(2, number)
                target[rows] = (base[rows].astype(jnp.float32) + total).astype(target.dtype)


class Weights:
    def __init__(self, at, link, chunks, moves):
        self.at, self.link, self.chunks, self.moves = at, link, chunks, moves

    def spread(self, number, k, only):
        at, (leaving, landing, extra) = self.at, self.chunks[number]
        owner = at.order[k]
        if extra:
            if k == 3 or k == 1 and only is at.is_inner:
                return
            only = at.is_outer if k == 1 else only
        self.link.send(
            leaving(owner, at.plane),
            landing(at.place, at.plane),
            self.moves.at[number, 0, at.place],
            {"fs": owner},
            only,
        )

    def forward(self, number, k):
        at, (_, landing, extra) = self.at, self.chunks[number]
        source, peer = at.sooner[k], {"grp": 1 - at.plane}
        here = landing(source, at.plane)

        def arrived():
            arrive(here, self.moves.at[number, 0, source], peer)

        only = at.is_inner if extra else None
        if only is None:
            arrived()
        else:
            pl.when(only)(arrived)
        self.link.send(here, here, self.moves.at[number, 1, source], peer, only)

    def wait(self, number):
        at, (_, landing, extra) = self.at, self.chunks[number]

        def arrived():
            for source in at.order[1:]:
                arrive(
                    landing(source, 1 - at.plane),
                    self.moves.at[number, 1, source],
                    {"grp": 1 - at.plane},
                )

        if extra:
            pl.when(at.is_inner)(arrived)
        else:
            arrived()


def recurrence(both, taps, decay_map, input_map, rate, extra):
    wide = jnp.float32
    size = both.shape[1] // 2
    block = decay_map[0].shape[1]
    recur = both[:, size:].astype(jnp.bfloat16).astype(wide)
    length = recur.shape[0]
    position = lax.broadcasted_iota(jnp.int32, recur.shape, 0)
    count = taps.shape[0]
    conv = recur * taps[count - 1 : count].astype(wide)
    for tap in range(count - 1):
        back = count - 1 - tap
        earlier = jnp.where(position >= back, pltpu.roll(recur, back, 0), 0.0)
        conv = conv + earlier * taps[tap : tap + 1].astype(wide)
    conv_rows = conv.astype(jnp.bfloat16)

    def mapped(matrix):
        products = [
            jnp.dot(
                conv_rows[:, n * block : (n + 1) * block], matrix[n], preferred_element_type=wide
            )
            for n in range(size // block)
        ]
        return jax.nn.sigmoid(jnp.concatenate(products, axis=1))

    recur_gate, input_rate = mapped(decay_map), mapped(input_map)
    log_decay = rate * recur_gate + extra
    decay = jnp.exp(log_decay)
    spread = -jnp.tanh(log_decay) * (decay * decay + 1.0)
    drive = jnp.sqrt(spread) * input_rate * conv_rows.astype(wide)
    back = 1
    while back < length:
        inside = position >= back
        drive = drive + decay * jnp.where(inside, pltpu.roll(drive, back, 0), 0.0)
        if back * 2 < length:
            decay = decay * jnp.where(inside, pltpu.roll(decay, back, 0), 1.0)
        back *= 2
    gate_rows = jax.nn.gelu(both[:, :size]).astype(jnp.bfloat16)
    return (drive * gate_rows.astype(wide)).astype(jnp.bfloat16)


def layer_kernel(
    tokens, gain_one, gain_two, taps, decay_map, input_map, logit, extra_own,
    gate, recur, outward, upward, downward, out,
    held_one, held_two, residual, normed, mixed, squared, both_w, out_w, up_w, down_w, extra,
    terms, from_core, to_x, from_x, to_z, from_z,
    pool, arrived, core_sems, x_sems, z_sems, moves, extra_sems, local_sems,
):
    at = Where()
    greet(at)
    link = Link(pool)
    length, width = tokens.shape
    depth, size = gate.shape[0], taps.shape[1] // 2
    most = up_w.shape[1]
    least = upward.shape[1] // 2 - most
    half, place = depth // 2, at.place

    def spot(start, count, step):
        return pl.ds(pl.multiple_of(start, step), count)

    def by_rows(weight, joined, columns, first, begins, extra=False):
        def leaving(owner, plane):
            return weight.at[spot(plane * half, half, half), spot(begins(owner), columns, 128)]

        def landing(source, plane):
            rows = spot(source * depth + plane * half, half, half)
            return joined.at[rows, pl.ds(first, columns)]

        return leaving, landing, extra

    def by_columns(weight, joined, rows_of, first, begins, extra=False):
        share = rows_of // 2

        def leaving(owner, plane):
            return weight.at[spot(begins(owner) + plane * share, share, 64)]

        def landing(source, plane):
            rows = spot(first + plane * share, share, 64)
            return joined.at[rows, spot(source * width, width, width)]

        return leaving, landing, extra

    def of_pair(owner):
        return lax.rem(owner, 2) * size

    def basic(owner):
        return owner * least + (owner + 1) // 3 * (most - least) + owner // 3 * (most - least)

    def further(owner):
        return basic(owner) + least

    chunks = [
        by_rows(gate, both_w, size, 0, of_pair),
        by_rows(recur, both_w, size, size, of_pair),
        by_columns(outward, out_w, size, 0, of_pair),
        by_rows(upward, up_w, least, 0, basic),
        by_rows(upward, up_w, most - least, least, further, True),
        by_columns(downward, down_w, least, 0, basic),
        by_columns(downward, down_w, most - least, least, further, True),
    ]
    weights = Weights(at, link, chunks, moves)

    def spread(numbers, ks=(1, 2, 3), only=None):
        for k in ks:
            for number in numbers:
                weights.spread(number, k, only)

    def forward(numbers, ks=(1, 2, 3)):
        for k in ks:
            for number in numbers:
                weights.forward(number, k)

    first = Gather(at, link, True, tokens, held_one, arrived.at[0])
    spread((0, 1), (1,))
    first.begin()
    spread((0, 1), (2, 3))
    link.send(extra_own.at[0], extra.at[place], extra_sems.at[place], {"fs": at.near})
    extra[place] = extra_own[0]
    local = []
    for number, (leaving, landing, extra_part) in enumerate(chunks):
        for plane in range(2):
            moving = pltpu.make_async_copy(
                leaving(place, plane), landing(place, plane), local_sems.at[number, plane]
            )
            local.append((moving, extra_part))
            if extra_part:
                pl.when(at.is_inner)(moving.start)
            else:
                moving.start()
    held_one[place, at.row] = tokens[...]
    first.cross(0)
    first.normalise(0, gain_one, normed.at[0])
    forward((0, 1), (1,))
    first.relay(1)
    spread((2,))
    forward((0, 1), (2,))
    first.cross(1)
    first.normalise(1, gain_one, normed.at[1])
    arrive(extra.at[at.near], extra_sems.at[at.near], {"fs": at.near})
    for moving, extra_part in local:
        if extra_part:
            pl.when(at.is_inner)(moving.wait)
        else:
            moving.wait()
    forward((0, 1), (3,))
    forward((2,), (1,))
    spread(UP)
    for number in range(2):
        weights.wait(number)
    side = lax.rem(place, 2)
    blocks = size // decay_map.shape[1]
    own_taps = taps[:, spot(side * size, size, size)]
    own_logit = logit[:, spot(side * size, size, size)]
    rate = -8.0 * (
        jnp.maximum(-own_logit, 0.0) + jnp.log1p(jnp.exp(-jnp.abs(own_logit)))
    )

    def mix(k):
        both = jnp.dot(normed[k], both_w[...], preferred_element_type=jnp.float32)
        added = jnp.transpose(jnp.broadcast_to(extra[at.order[k]], (size, length)))
        maps = [
            [matrix[side * blocks + n] for n in range(blocks)] for matrix in (decay_map, input_map)
        ]
        mixed[k] = recurrence(both, own_taps, *maps, rate, added)

    def project(k):
        for part in range(4):
            terms[0, k, part] = jnp.dot(
                mixed[k], out_w[:, pl.ds(part * width, width)], preferred_element_type=jnp.float32
            ).astype(terms.dtype)

    def scatter(turn):
        return Scatter(
            at, link, not turn, terms.at[turn], from_core.at[turn], to_x.at[turn], from_x.at[turn],
            to_z.at[turn], from_z.at[turn],
            (core_sems.at[turn], x_sems.at[turn], z_sems.at[turn]),
        )

    summed = scatter(0)
    mix(1)
    forward((2,), (2,))
    mix(0)
    forward((2,), (3,))
    weights.wait(2)
    project(1)
    summed.core(1)
    project(0)
    summed.core(0)
    summed.x(1)
    summed.x(0)
    summed.z(1)
    forward(UP[:1])
    summed.own(tokens, residual)

    second = Gather(at, link, False, residual, held_two, arrived.at[1])
    second.begin()
    held_two[place, at.row] = residual[...]
    forward(UP[1:], (1,))
    second.relay(1)
    spread(DOWN[:1], (2, 3), at.is_inner)
    spread(DOWN[:1], (1, 2, 3), at.is_outer)
    second.cross(0)
    second.relay(2)
    spread(DOWN[:1], (1,), at.is_inner)
    spread(DOWN[1:], (1, 2, 3), at.is_outer)
    second.cross(1)
    second.normalise(0, gain_two, normed.at[0])
    forward(UP[1:], (2, 3))
    second.relay(3)
    spread(DOWN[1:], (1, 2, 3), at.is_inner)
    second.cross(2)
    forward(DOWN[:1], (1,))
    second.normalise(1, gain_two, normed.at[1])
    forward(DOWN[:1], (2, 3))
    second.normalise(2, gain_two, normed.at[2])
    second.cross(3)
    second.normalise(3, gain_two, normed.at[3])
    for number in UP:
        weights.wait(number)
    forward(DOWN[1:], (1,))
    def raised(k, columns):
        product = jnp.dot(normed[k], up_w[:, columns], preferred_element_type=jnp.float32)
        positive = jnp.maximum(product, 0.0)
        squared[k, :, columns] = (positive * positive).astype(squared.dtype)

    def lift(k):
        raised(k, pl.ds(0, least))

        @pl.when(at.is_inner)
        def _():
            raised(k, pl.ds(least, most - least))

    def lowered(k, count):
        for part in range(4):
            terms[1, k, part] = jnp.dot(
                squared[k, :, pl.ds(0, count)],
                down_w[pl.ds(0, count), pl.ds(part * width, width)],
                preferred_element_type=jnp.float32,
            ).astype(terms.dtype)

    def lower(k):
        @pl.when(at.is_inner)
        def _():
            lowered(k, most)

        @pl.when(at.is_outer)
        def _():
            lowered(k, least)

    last = scatter(1)
    lift(3)
    lift(2)
    forward(DOWN[1:], (2,))
    lift(1)
    lift(0)
    forward(DOWN[1:], (3,))
    for number in DOWN:
        weights.wait(number)
    lower(3)
    last.core(3)
    lower(2)
    last.core(2)
    last.x(3)
    lower(1)
    last.core(1)
    last.x(2)
    lower(0)
    last.core(0)
    last.x(1)
    last.x(0)
    last.z(3)
    last.z(2)
    last.z(1)
    last.own(residual, out)
    link.finish()


def per_device_owned(
    tokens,
    recurrent_norm_gain,
    feedforward_norm_gain,
    gate_projection_weight,
    recurrent_projection_weight,
    convolution_kernel,
    decay_gate_matrix,
    input_gate_matrix,
    base_decay_logit,
    extra_log_decay,
    output_projection_weight,
    up_projection_weight,
    down_projection_weight,
):
    length, width = tokens.shape
    depth, size = gate_projection_weight.shape[0], gate_projection_weight.shape[1] // 2
    hidden = up_projection_weight.shape[1] // 4
    hidden += hidden // 4
    kind, wide = tokens.dtype, jnp.float32
    vmem, anywhere = pl.BlockSpec(memory_space=pltpu.VMEM), pl.BlockSpec(memory_space=pltpu.HBM)
    dma, block = pltpu.SemaphoreType.DMA, (length, width)
    scratch = [
        ((4, 4) + block, kind),
        ((4, 4) + block, kind),
        (block, kind),
        ((4, length, 4 * width), kind),
        ((4, length, size), kind),
        ((4, length, hidden), kind),
        ((4 * depth, 2 * size), kind),
        ((size, 4 * width), kind),
        ((4 * depth, hidden), kind),
        ((hidden, 4 * width), kind),
        ((4, 1, length), wide),
        ((2, 4, 4) + block, kind),
        ((2, 2, 4) + block, kind),
        ((2, 4) + block, kind),
        ((2, 4) + block, kind),
        ((2, 4) + block, kind),
        ((2, 5) + block, kind),
    ]
    return pl.pallas_call(
        layer_kernel,
        out_shape=jax.ShapeDtypeStruct(block, kind),
        in_specs=[vmem] * 8 + [anywhere] * 5,
        out_specs=vmem,
        scratch_shapes=[pltpu.VMEM(*entry) for entry in scratch]
        + [
            dma((POOL,)),
            dma((2, 4, 4, PIECES)),
            dma((2, 2, 4)),
            dma((2, 4, PIECES)),
            dma((2, 5, PIECES)),
            dma((7, 2, 4)),
            dma((4,)),
            dma((7, 2)),
        ],
        compiler_params=pltpu.CompilerParams(
            collective_id=1, has_side_effects=True, vmem_limit_bytes=LIMIT
        ),
    )(
        tokens,
        recurrent_norm_gain.reshape(1, -1),
        feedforward_norm_gain.reshape(1, -1),
        convolution_kernel,
        decay_gate_matrix,
        input_gate_matrix,
        base_decay_logit.reshape(1, -1),
        extra_log_decay.reshape(1, 1, -1),
        gate_projection_weight,
        recurrent_projection_weight,
        output_projection_weight,
        up_projection_weight,
        down_projection_weight,
    )


def solution(mesh):
    placed = (
        P(("grp", "fs"), "tp"),
        P(),
        P(),
        P("fs", "tp"),
        P("fs", "tp"),
        P(None, "tp"),
        P("tp", None, None),
        P("tp", None, None),
        P("tp"),
        P(("grp", "fs")),
        P("tp", "fs"),
        P("fs", "tp"),
        P("tp", "fs"),
    )
    owners = mesh.shape["fs"] * mesh.shape["tp"]
    fitting = mesh.shape["tp"] == 4 and mesh.shape["grp"] == 2 and mesh.shape["fs"] == 4

    def run(*arrays):
        owned = fitting and arrays[6].shape[0] == owners
        body = per_device_owned if owned else per_device
        return jax.shard_map(
            body, mesh=mesh, in_specs=placed, out_specs=P(("grp", "fs"), "tp"), check_vma=False
        )(*arrays)

    return run
```

```python
import functools

import jax
import jax.numpy as jnp
from jax import lax
from jax.experimental import pallas as pl
from jax.experimental.pallas import tpu as pltpu
from jax.sharding import PartitionSpec as P

MESH = pl.DeviceIdType.MESH


def rms_rows(values_in, norm_gain):
    values = values_in.astype(jnp.float32)
    inverse = lax.rsqrt(jnp.mean(values * values, axis=-1, keepdims=True) + 1e-06)
    return (values * inverse * norm_gain).astype(jnp.bfloat16)


def combine(earlier, later):
    return (earlier[0] * later[0], later[0] * earlier[1] + later[1])


def recurrent_state(
    recurrent_branch_rows,
    gate_branch_rows,
    convolution_kernel,
    decay_gate_matrix,
    input_gate_matrix,
    base_decay_logit,
    extra_log_decay,
):
    length = recurrent_branch_rows.shape[0]
    taps = convolution_kernel.shape[0]
    padded = jnp.pad(recurrent_branch_rows.astype(jnp.float32), ((taps - 1, 0), (0, 0)))
    conv_sum = jnp.zeros((length, recurrent_branch_rows.shape[1]), jnp.float32)
    for tap_index in range(taps):
        conv_sum = conv_sum + padded[tap_index : tap_index + length] * convolution_kernel[
            tap_index
        ].astype(jnp.float32)
    conv_rows = conv_sum.astype(jnp.bfloat16)
    blocks = decay_gate_matrix.shape[0]
    blocked = conv_rows.reshape(length, blocks, -1)
    recurrence_gate = jax.nn.sigmoid(
        jnp.einsum(
            "tni,nij->tnj", blocked, decay_gate_matrix, preferred_element_type=jnp.float32
        ).reshape(length, -1)
    )
    input_rate = jax.nn.sigmoid(
        jnp.einsum(
            "tni,nij->tnj", blocked, input_gate_matrix, preferred_element_type=jnp.float32
        ).reshape(length, -1)
    )
    decay_log_values = (
        -8.0 * jax.nn.softplus(-base_decay_logit) * recurrence_gate + extra_log_decay[:, None]
    )
    decay = jnp.exp(decay_log_values)
    drive = (
        jnp.sqrt(-jnp.expm1(2.0 * decay_log_values)) * input_rate * conv_rows.astype(jnp.float32)
    )
    _, hidden = lax.associative_scan(combine, (decay, drive), axis=0)
    return (hidden * gate_branch_rows.astype(jnp.float32)).astype(jnp.bfloat16)


def per_device(
    tokens,
    recurrent_norm_gain,
    feedforward_norm_gain,
    gate_projection_weight,
    recurrent_projection_weight,
    convolution_kernel,
    decay_gate_matrix,
    input_gate_matrix,
    base_decay_logit,
    extra_log_decay,
    output_projection_weight,
    up_projection_weight,
    down_projection_weight,
):
    whole_rows = lax.all_gather(tokens, "tp", axis=1, tiled=True)
    normed = rms_rows(whole_rows, recurrent_norm_gain)
    columns = normed
    gate_pre = jnp.dot(
        columns,
        lax.all_gather(gate_projection_weight, "fs", axis=0, tiled=True),
        preferred_element_type=jnp.float32,
    )
    recur_pre = jnp.dot(
        columns,
        lax.all_gather(recurrent_projection_weight, "fs", axis=0, tiled=True),
        preferred_element_type=jnp.float32,
    )
    gate_branch_rows = jax.nn.gelu(gate_pre).astype(jnp.bfloat16)
    recurrent_branch_rows = recur_pre.astype(jnp.bfloat16)
    mixed_output = recurrent_state(
        recurrent_branch_rows,
        gate_branch_rows,
        convolution_kernel,
        decay_gate_matrix,
        input_gate_matrix,
        base_decay_logit,
        extra_log_decay,
    )
    partials = jnp.dot(
        mixed_output,
        lax.all_gather(output_projection_weight, "fs", axis=1, tiled=True),
        preferred_element_type=jnp.float32,
    )
    residual = (
        tokens.astype(jnp.float32)
        + lax.psum_scatter(
            partials.astype(jnp.bfloat16), "tp", scatter_dimension=1, tiled=True
        ).astype(jnp.float32)
    ).astype(jnp.bfloat16)
    middle = lax.all_gather(residual, "tp", axis=1, tiled=True)
    channel_in = rms_rows(middle, feedforward_norm_gain)
    columns = channel_in
    upward = jnp.dot(
        columns,
        lax.all_gather(up_projection_weight, "fs", axis=0, tiled=True),
        preferred_element_type=jnp.float32,
    )
    positive = jnp.maximum(upward, 0.0)
    squared = (positive * positive).astype(jnp.bfloat16)
    down_terms = jnp.dot(
        squared,
        lax.all_gather(down_projection_weight, "fs", axis=1, tiled=True),
        preferred_element_type=jnp.float32,
    )
    summed_down = lax.psum_scatter(
        down_terms.astype(jnp.bfloat16), "tp", scatter_dimension=1, tiled=True
    ).astype(jnp.float32)
    return (residual.astype(jnp.float32) + summed_down).astype(jnp.bfloat16)

PIECES = 2
POOL = 56
UP, DOWN = (3, 4), (5, 6)
LIMIT = 58 * 2**20
TILE = 64


class Link:
    def __init__(self, pool):
        self.pool, self.started = pool, []

    def drain(self, moving, only):
        if only is None:
            moving.wait_send()
        else:
            pl.when(only)(moving.wait_send)

    def send(self, source, target, arrival, peer, only=None):
        turn = len(self.started)
        if turn >= POOL:
            self.drain(*self.started[turn - POOL])
        moving = pltpu.make_async_remote_copy(
            src_ref=source,
            dst_ref=target,
            send_sem=self.pool.at[turn % POOL],
            recv_sem=arrival,
            device_id=peer,
            device_id_type=MESH,
        )
        self.started.append((moving, only))
        if only is None:
            moving.start()
        else:
            pl.when(only)(moving.start)

    def finish(self):
        for moving, only in self.started[-POOL:]:
            self.drain(moving, only)


def arrive(target, arrival, peer):
    pltpu.make_async_remote_copy(
        src_ref=target,
        dst_ref=target,
        send_sem=arrival,
        recv_sem=arrival,
        device_id=peer,
        device_id_type=MESH,
    ).wait_recv()


class Where:
    def __init__(self):
        self.place, self.row = lax.axis_index("fs"), lax.axis_index("tp")
        self.plane = lax.axis_index("grp")
        place = self.place
        self.near = place + 1 - 2 * lax.rem(place, 2)
        self.mid = 3 - place
        self.inner = lax.rem((place + 1) // 2, 2)
        self.is_inner, self.is_outer = self.inner == 1, self.inner == 0
        far = place // 2
        self.order = [place, self.near, 2 - far, 3 - 3 * far]
        near, other = self.near, self.order[2]
        self.sooner = [place, near + self.inner * (other - near)]
        self.sooner += [other + self.inner * (near - other), self.order[3]]
        self.across, self.beside, self.corner = self.row ^ 2, self.row ^ 1, self.row ^ 3


def greet(at):
    barrier = pltpu.get_barrier_semaphore()
    peers = [{"fs": spot} for spot in at.order[1:]]
    peers += [{"tp": at.beside}, {"tp": at.across}, {"grp": 1 - at.plane}]
    for peer in peers:
        pl.semaphore_signal(barrier, inc=1, device_id=peer, device_id_type=MESH)
    pl.semaphore_wait(barrier, len(peers))


class Gather:
    def __init__(self, at, link, pair, own, held, arrived):
        self.at, self.link, self.own, self.held, self.arrived = at, link, own, held, arrived
        self.pair = pair
        self.step = own.shape[0] // PIECES

    def piece(self, origin, part, number):
        return self.held.at[origin, part, pl.ds(number * self.step, self.step)]

    def send(self, source, origin, part, number, peer, only=None):
        self.link.send(
            source,
            self.piece(origin, part, number),
            self.arrived.at[origin, part, number],
            peer,
            only,
        )

    def wait(self, origin, part, number):
        arrive(
            self.piece(origin, part, number),
            self.arrived.at[origin, part, number],
            {"tp": self.at.beside},
        )

    def begin(self, along=True, aside=True):
        at = self.at
        for number in range(PIECES):
            source = self.own.at[pl.ds(number * self.step, self.step)]
            if along:
                self.send(source, at.place, at.row, number, {"fs": at.near})
                if not self.pair:
                    self.send(source, at.place, at.row, number, {"fs": at.mid}, at.is_inner)
            if aside:
                self.send(source, at.place, at.row, number, {"tp": at.across})
                self.send(source, at.place, at.row, number, {"tp": at.beside})

    def relay(self, k):
        at, origin = self.at, self.at.order[k]
        for number in range(PIECES):
            self.wait(origin, at.row, number)
            source = self.piece(origin, at.row, number)
            onward = {"fs": at.mid if k == 1 else at.near}
            if not self.pair:
                self.send(source, origin, at.row, number, onward, at.is_inner)
            self.send(source, origin, at.row, number, {"tp": at.across})
            self.send(source, origin, at.row, number, {"tp": at.beside})

    def cross(self, k):
        at, origin = self.at, self.at.order[k]
        for number in range(PIECES):
            self.wait(origin, at.across, number)
            source = self.piece(origin, at.across, number)
            self.send(source, origin, at.across, number, {"tp": at.beside})

    def normalise(self, k, norm_gain, target):
        at, origin = self.at, self.at.order[k]
        for number in range(PIECES):
            self.wait(origin, at.beside, number)
            self.wait(origin, at.corner, number)
        length, width = self.own.shape
        parts_of = self.held.shape[1]

        def tile(index, carry):
            rows = pl.ds(pl.multiple_of(index * TILE, TILE), TILE)
            parts = [self.held[origin, p, rows].astype(jnp.float32) for p in range(parts_of)]
            total = sum(jnp.sum(part * part, axis=-1, keepdims=True) for part in parts)
            inverse = lax.rsqrt(total / (parts_of * width) + 1e-06)
            for number, part in enumerate(parts):
                columns = pl.ds(number * width, width)
                target[rows, columns] = (part * inverse * norm_gain[:, columns]).astype(
                    target.dtype
                )
            return carry

        lax.fori_loop(0, length // TILE, tile, 0)


class Scatter:
    def __init__(self, at, link, pair, terms, from_core, to_x, from_x, to_z, from_z, sems):
        self.pair = pair
        self.at, self.link, self.terms = at, link, terms
        self.from_core, self.to_x, self.from_x = from_core, to_x, from_x
        self.to_z, self.from_z = to_z, from_z
        self.core_sems, self.x_sems, self.z_sems = sems
        self.step = terms.shape[2] // PIECES

    def rows(self, number):
        return pl.ds(number * self.step, self.step)

    def core(self, k):
        at = self.at
        for side, part in ((1, at.corner), (0, at.beside)):
            self.link.send(
                self.terms.at[k, part],
                self.from_core.at[side, k],
                self.core_sems.at[side, k],
                {"tp": at.beside},
            )

    def x(self, k):
        at = self.at
        arrive(self.from_core.at[1, k], self.core_sems.at[1, k], {"tp": at.beside})
        for number in range(PIECES):
            rows = self.rows(number)
            mine = self.terms[k, at.across, rows].astype(jnp.float32)
            theirs = self.from_core[1, k, rows].astype(jnp.float32)
            self.to_x[k, rows] = (mine + theirs).astype(self.to_x.dtype)
            self.link.send(
                self.to_x.at[k, rows],
                self.from_x.at[k, rows],
                self.x_sems.at[k, number],
                {"tp": at.across},
            )

    def joined(self, k, number):
        rows = self.rows(number)
        mine = self.terms[k, self.at.row, rows].astype(jnp.float32)
        mine = mine + self.from_core[0, k, rows].astype(jnp.float32)
        return mine + self.from_x[k, rows].astype(jnp.float32)

    def taken(self, slot, number):
        rows = self.rows(number)
        arrive(
            self.from_z.at[slot, rows], self.z_sems.at[slot, number], {"fs": self.at.near}
        )
        return self.from_z[slot, rows].astype(jnp.float32)

    def ready(self, k, number):
        at, rows = self.at, self.rows(number)
        if not number:
            arrive(self.from_core.at[0, k], self.core_sems.at[0, k], {"tp": at.beside})
        arrive(self.from_x.at[k, rows], self.x_sems.at[k, number], {"tp": at.across})

    def z(self, k):
        at = self.at
        comes = {2: 0, 3: 1, 1: 4}[k]
        if self.pair:
            for number in range(PIECES):
                rows = self.rows(number)
                self.ready(k, number)
                self.to_z[k, rows] = self.joined(k, number).astype(self.to_z.dtype)
                self.link.send(
                    self.to_z.at[k, rows],
                    self.from_z.at[2, rows],
                    self.z_sems.at[2, number],
                    {"fs": at.near},
                )
            return
        peer = at.near if k == 1 else at.near + at.inner * (at.mid - at.near)
        slot = {2: 3 * at.inner, 3: 1 + 3 * at.inner, 1: 2}[k]
        for number in range(PIECES):
            rows = self.rows(number)
            self.ready(k, number)

            @pl.when(at.is_inner)
            def _():
                total = self.joined(k, number) + self.taken(comes, number)
                self.to_z[k, rows] = total.astype(self.to_z.dtype)

            @pl.when(at.is_outer)
            def _():
                self.to_z[k, rows] = self.joined(k, number).astype(self.to_z.dtype)

            self.link.send(
                self.to_z.at[k, rows],
                self.from_z.at[slot, rows],
                self.z_sems.at[slot, number],
                {"fs": peer},
            )

    def own(self, base, target):
        at = self.at
        for number in range(PIECES):
            rows = self.rows(number)
            self.ready(0, number)
            if self.pair:
                total = self.joined(0, number) + self.taken(2, number)
                target[rows] = (base[rows].astype(jnp.float32) + total).astype(target.dtype)
                continue

            @pl.when(at.is_inner)
            def _():
                total = self.joined(0, number) + self.taken(2, number) + self.taken(3, number)
                target[rows] = (base[rows].astype(jnp.float32) + total).astype(target.dtype)

            @pl.when(at.is_outer)
            def _():
                total = self.joined(0, number) + self.taken(2, number)
                target[rows] = (base[rows].astype(jnp.float32) + total).astype(target.dtype)


class Weights:
    def __init__(self, at, link, chunks, moves):
        self.at, self.link, self.chunks, self.moves = at, link, chunks, moves

    def spread(self, number, k, only):
        at, (leaving, landing, extra) = self.at, self.chunks[number]
        owner = at.order[k]
        if extra:
            if k == 3 or k == 1 and only is at.is_inner:
                return
            only = at.is_outer if k == 1 else only
        self.link.send(
            leaving(owner, at.plane),
            landing(at.place, at.plane),
            self.moves.at[number, 0, at.place],
            {"fs": owner},
            only,
        )

    def forward(self, number, k, only):
        at, (_, landing, extra) = self.at, self.chunks[number]
        source, peer = at.sooner[k], {"grp": 1 - at.plane}
        here = landing(source, at.plane)

        def arrived():
            arrive(here, self.moves.at[number, 0, source], peer)

        if extra and only is at.is_outer:
            return
        only = at.is_inner if extra else only
        if only is None:
            arrived()
        else:
            pl.when(only)(arrived)
        self.link.send(here, here, self.moves.at[number, 1, source], peer, only)

    def wait(self, number):
        at, (_, landing, extra) = self.at, self.chunks[number]

        def arrived():
            for source in at.order[1:]:
                arrive(
                    landing(source, 1 - at.plane),
                    self.moves.at[number, 1, source],
                    {"grp": 1 - at.plane},
                )

        if extra:
            pl.when(at.is_inner)(arrived)
        else:
            arrived()


def recurrence(both, taps, decay_map, input_map, rate, extra):
    wide = jnp.float32
    size = both.shape[1] // 2
    block = decay_map[0].shape[1]
    recur = both[:, size:].astype(jnp.bfloat16).astype(wide)
    length = recur.shape[0]
    position = lax.broadcasted_iota(jnp.int32, recur.shape, 0)
    count = taps.shape[0]
    conv = recur * taps[count - 1 : count].astype(wide)
    for tap in range(count - 1):
        back = count - 1 - tap
        earlier = jnp.where(position >= back, pltpu.roll(recur, back, 0), 0.0)
        conv = conv + earlier * taps[tap : tap + 1].astype(wide)
    conv_rows = conv.astype(jnp.bfloat16)

    def mapped(matrix):
        products = [
            jnp.dot(
                conv_rows[:, n * block : (n + 1) * block], matrix[n], preferred_element_type=wide
            )
            for n in range(size // block)
        ]
        return jax.nn.sigmoid(jnp.concatenate(products, axis=1))

    recur_gate, input_rate = mapped(decay_map), mapped(input_map)
    log_decay = rate * recur_gate + extra
    decay = jnp.exp(log_decay)
    spread = -jnp.tanh(log_decay) * (decay * decay + 1.0)
    drive = jnp.sqrt(spread) * input_rate * conv_rows.astype(wide)
    back = 1
    while back < length:
        inside = position >= back
        drive = drive + decay * jnp.where(inside, pltpu.roll(drive, back, 0), 0.0)
        if back * 2 < length:
            decay = decay * jnp.where(inside, pltpu.roll(decay, back, 0), 1.0)
        back *= 2
    gate_rows = jax.nn.gelu(both[:, :size]).astype(jnp.bfloat16)
    return (drive * gate_rows.astype(wide)).astype(jnp.bfloat16)


def layer_kernel(
    tokens_from, gain_one_from, gain_two_from, taps_from, decay_map_from, input_map_from,
    logit_from, extra_from, gate, recur, outward, upward, downward, out,
    held_one, held_two, residual, normed, mixed, squared, both_w, out_w, up_w, down_w, extra,
    terms, from_core, to_x, from_x, to_z, from_z,
    tokens, gain_one, gain_two, taps, decay_map, input_map, logit, extra_own,
    small_sems, pool, arrived, core_sems, x_sems, z_sems, moves, extra_sems, local_sems,
):
    at = Where()
    small = []
    for number, (source, target) in enumerate(
        (
            (tokens_from, tokens), (extra_from, extra_own), (gain_one_from, gain_one),
            (taps_from, taps), (decay_map_from, decay_map), (input_map_from, input_map),
            (logit_from, logit), (gain_two_from, gain_two),
        )
    ):
        small.append(pltpu.make_async_copy(source, target, small_sems.at[number]))
        small[-1].start()
    greet(at)
    for moving in small:
        moving.wait()
    link = Link(pool)
    length, width = tokens.shape
    depth, size = gate.shape[0], taps.shape[1] // 2
    most = up_w.shape[1]
    least = upward.shape[1] // 2 - most
    half, place = depth // 2, at.place

    def spot(start, count, step):
        return pl.ds(pl.multiple_of(start, step), count)

    def by_rows(weight, joined, columns, first, begins, extra=False):
        def leaving(owner, plane):
            return weight.at[spot(plane * half, half, half), spot(begins(owner), columns, 128)]

        def landing(source, plane):
            rows = spot(source * depth + plane * half, half, half)
            return joined.at[rows, pl.ds(first, columns)]

        return leaving, landing, extra

    def by_columns(weight, joined, rows_of, first, begins, extra=False):
        share = rows_of // 2

        def leaving(owner, plane):
            return weight.at[spot(begins(owner) + plane * share, share, 64)]

        def landing(source, plane):
            rows = spot(first + plane * share, share, 64)
            return joined.at[rows, spot(source * width, width, width)]

        return leaving, landing, extra

    def of_pair(owner):
        return lax.rem(owner, 2) * size

    def basic(owner):
        return owner * least + (owner + 1) // 3 * (most - least) + owner // 3 * (most - least)

    def further(owner):
        return basic(owner) + least

    chunks = [
        by_rows(gate, both_w, size, 0, of_pair),
        by_rows(recur, both_w, size, size, of_pair),
        by_columns(outward, out_w, size, 0, of_pair),
        by_rows(upward, up_w, least, 0, basic),
        by_rows(upward, up_w, most - least, least, further, True),
        by_columns(downward, down_w, least, 0, basic),
        by_columns(downward, down_w, most - least, least, further, True),
    ]
    weights = Weights(at, link, chunks, moves)

    def spread(numbers, ks=(1, 2, 3), only=None):
        for k in ks:
            for number in numbers:
                weights.spread(number, k, only)

    def forward(numbers, ks=(1, 2, 3), only=None):
        for k in ks:
            for number in numbers:
                weights.forward(number, k, only)

    first = Gather(at, link, True, tokens, held_one, arrived)
    spread((0, 1), (1,))
    first.begin()
    spread((0, 1), (2, 3))
    link.send(extra_own.at[0], extra.at[place], extra_sems.at[place], {"fs": at.near})
    extra[place] = extra_own[0]
    local = []
    for number, (leaving, landing, extra_part) in enumerate(chunks):
        for plane in range(2):
            moving = pltpu.make_async_copy(
                leaving(place, plane), landing(place, plane), local_sems.at[number, plane]
            )
            local.append((moving, extra_part))
            if extra_part:
                pl.when(at.is_inner)(moving.start)
            else:
                moving.start()
    held_one[place, at.row] = tokens[...]
    first.cross(0)
    first.normalise(0, gain_one, normed.at[0])
    forward((0, 1), (1,))
    first.relay(1)
    spread((2,))
    forward((0, 1), (2,))
    first.cross(1)
    first.normalise(1, gain_one, normed.at[1])
    arrive(extra.at[at.near], extra_sems.at[at.near], {"fs": at.near})
    for moving, extra_part in local:
        if extra_part:
            pl.when(at.is_inner)(moving.wait)
        else:
            moving.wait()
    forward((0, 1), (3,))
    forward((2,), (1,))
    for number in range(2):
        weights.wait(number)
    spread(UP)
    side = lax.rem(place, 2)
    blocks = size // decay_map.shape[1]
    own_taps = taps[:, spot(side * size, size, size)]
    own_logit = logit[:, spot(side * size, size, size)]
    rate = -8.0 * (
        jnp.maximum(-own_logit, 0.0) + jnp.log1p(jnp.exp(-jnp.abs(own_logit)))
    )

    def mix(k):
        both = jnp.dot(normed[k], both_w[...], preferred_element_type=jnp.float32)
        added = jnp.transpose(jnp.broadcast_to(extra[at.order[k]], (size, length)))
        maps = [
            [matrix[side * blocks + n] for n in range(blocks)] for matrix in (decay_map, input_map)
        ]
        mixed[k] = recurrence(both, own_taps, *maps, rate, added)

    def project(k):
        for part in range(4):
            terms[0, k, part] = jnp.dot(
                mixed[k], out_w[:, pl.ds(part * width, width)], preferred_element_type=jnp.float32
            ).astype(terms.dtype)

    def scatter(turn):
        return Scatter(
            at, link, not turn, terms.at[turn], from_core.at[turn], to_x.at[turn], from_x.at[turn],
            to_z.at[turn], from_z.at[turn],
            (core_sems, x_sems, z_sems),
        )

    summed = scatter(0)
    mix(1)
    forward((2,), (2,))
    mix(0)
    forward((2,), (3,))
    weights.wait(2)
    project(1)
    summed.core(1)
    project(0)
    summed.core(0)
    summed.x(1)
    summed.x(0)
    summed.z(1)
    spread(DOWN[:1], (2, 3, 1), at.is_inner)
    forward(UP[:1])
    spread(DOWN[:1], (1,), at.is_outer)
    summed.own(tokens, residual)

    second = Gather(at, link, False, residual, held_two, arrived)
    second.begin()
    spread(DOWN[1:], (1,), at.is_outer)
    held_two[place, at.row] = residual[...]
    forward(UP[1:])
    forward(DOWN[:1], (1,))
    second.relay(1)
    spread(DOWN[:1], (2, 3), at.is_outer)
    spread(DOWN[1:], (2,), at.is_outer)
    second.cross(0)
    second.relay(2)
    spread(DOWN[1:], (2,), at.is_inner)
    second.cross(1)
    forward(DOWN[:1], (2,))
    second.normalise(0, gain_two, normed.at[0])
    second.relay(3)
    second.cross(2)
    forward(DOWN[:1], (3,))
    forward(DOWN[1:], (2,))
    second.normalise(1, gain_two, normed.at[1])
    second.normalise(2, gain_two, normed.at[2])
    second.cross(3)
    forward(DOWN[1:], (1,))
    second.normalise(3, gain_two, normed.at[3])
    forward(DOWN[1:], (3,))
    for number in UP:
        weights.wait(number)
    def raised(k, columns):
        product = jnp.dot(normed[k], up_w[:, columns], preferred_element_type=jnp.float32)
        positive = jnp.maximum(product, 0.0)
        squared[k, :, columns] = (positive * positive).astype(squared.dtype)

    def lift(k):
        raised(k, pl.ds(0, least))

        @pl.when(at.is_inner)
        def _():
            raised(k, pl.ds(least, most - least))

    def lowered(k, count):
        for part in range(4):
            terms[1, k, part] = jnp.dot(
                squared[k, :, pl.ds(0, count)],
                down_w[pl.ds(0, count), pl.ds(part * width, width)],
                preferred_element_type=jnp.float32,
            ).astype(terms.dtype)

    def lower(k):
        @pl.when(at.is_inner)
        def _():
            lowered(k, most)

        @pl.when(at.is_outer)
        def _():
            lowered(k, least)

    last = scatter(1)
    lift(3)
    lift(2)
    lift(1)
    lift(0)
    for number in DOWN:
        weights.wait(number)
    lower(3)
    last.core(3)
    lower(2)
    last.core(2)
    last.x(3)
    lower(1)
    last.core(1)
    last.x(2)
    lower(0)
    last.core(0)
    last.x(1)
    last.x(0)
    last.z(3)
    last.z(2)
    last.z(1)
    last.own(residual, out)
    link.finish()


def per_device_owned(
    tokens,
    recurrent_norm_gain,
    feedforward_norm_gain,
    gate_projection_weight,
    recurrent_projection_weight,
    convolution_kernel,
    decay_gate_matrix,
    input_gate_matrix,
    base_decay_logit,
    extra_log_decay,
    output_projection_weight,
    up_projection_weight,
    down_projection_weight,
):
    length, width = tokens.shape
    depth, size = gate_projection_weight.shape[0], gate_projection_weight.shape[1] // 2
    hidden = up_projection_weight.shape[1] // 4
    hidden += hidden // 4
    kind, wide = tokens.dtype, jnp.float32
    vmem, anywhere = pl.BlockSpec(memory_space=pltpu.VMEM), pl.BlockSpec(memory_space=pltpu.HBM)
    dma, block = pltpu.SemaphoreType.DMA, (length, width)
    scratch = [
        ((4, 4) + block, kind),
        ((4, 4) + block, kind),
        (block, kind),
        ((4, length, 4 * width), kind),
        ((4, length, size), kind),
        ((4, length, hidden), kind),
        ((4 * depth, 2 * size), kind),
        ((size, 4 * width), kind),
        ((4 * depth, hidden), kind),
        ((hidden, 4 * width), kind),
        ((4, 1, length), wide),
        ((2, 4, 4) + block, kind),
        ((2, 2, 4) + block, kind),
        ((2, 4) + block, kind),
        ((2, 4) + block, kind),
        ((2, 4) + block, kind),
        ((2, 5) + block, kind),
        (block, kind),
        ((1, 4 * width), wide),
        ((1, 4 * width), wide),
        (convolution_kernel.shape, convolution_kernel.dtype),
        (decay_gate_matrix.shape, decay_gate_matrix.dtype),
        (input_gate_matrix.shape, input_gate_matrix.dtype),
        ((1, base_decay_logit.shape[0]), wide),
        ((1, 1, length), wide),
    ]
    return pl.pallas_call(
        layer_kernel,
        out_shape=jax.ShapeDtypeStruct(block, kind),
        in_specs=[anywhere] * 13,
        out_specs=vmem,
        scratch_shapes=[pltpu.VMEM(*entry) for entry in scratch]
        + [
            dma((8,)),
            dma((POOL,)),
            dma((4, 4, PIECES)),
            dma((2, 4)),
            dma((4, PIECES)),
            dma((5, PIECES)),
            dma((7, 2, 4)),
            dma((4,)),
            dma((7, 2)),
        ],
        compiler_params=pltpu.CompilerParams(
            collective_id=1, has_side_effects=True, vmem_limit_bytes=LIMIT
        ),
    )(
        tokens,
        recurrent_norm_gain.reshape(1, -1),
        feedforward_norm_gain.reshape(1, -1),
        convolution_kernel,
        decay_gate_matrix,
        input_gate_matrix,
        base_decay_logit.reshape(1, -1),
        extra_log_decay.reshape(1, 1, -1),
        gate_projection_weight,
        recurrent_projection_weight,
        output_projection_weight,
        up_projection_weight,
        down_projection_weight,
    )


def solution(mesh):
    placed = (
        P(("grp", "fs"), "tp"),
        P(),
        P(),
        P("fs", "tp"),
        P("fs", "tp"),
        P(None, "tp"),
        P("tp", None, None),
        P("tp", None, None),
        P("tp"),
        P(("grp", "fs")),
        P("tp", "fs"),
        P("fs", "tp"),
        P("tp", "fs"),
    )
    owners = mesh.shape["fs"] * mesh.shape["tp"]
    fitting = mesh.shape["tp"] == 4 and mesh.shape["grp"] == 2 and mesh.shape["fs"] == 4

    def run(*arrays):
        owned = fitting and arrays[6].shape[0] == owners
        body = per_device_owned if owned else per_device
        return jax.shard_map(
            body, mesh=mesh, in_specs=placed, out_specs=P(("grp", "fs"), "tp"), check_vma=False
        )(*arrays)

    return run
```

```python
import functools

import jax
import jax.numpy as jnp
from jax import lax
from jax.experimental import pallas as pl
from jax.experimental.pallas import tpu as pltpu
from jax.sharding import PartitionSpec as P

MESH = pl.DeviceIdType.MESH


def rms_rows(values_in, norm_gain):
    values = values_in.astype(jnp.float32)
    inverse = lax.rsqrt(jnp.mean(values * values, axis=-1, keepdims=True) + 1e-06)
    return (values * inverse * norm_gain).astype(jnp.bfloat16)


def combine(earlier, later):
    return (earlier[0] * later[0], later[0] * earlier[1] + later[1])


def recurrent_state(
    recurrent_branch_rows,
    gate_branch_rows,
    convolution_kernel,
    decay_gate_matrix,
    input_gate_matrix,
    base_decay_logit,
    extra_log_decay,
):
    length = recurrent_branch_rows.shape[0]
    taps = convolution_kernel.shape[0]
    padded = jnp.pad(recurrent_branch_rows.astype(jnp.float32), ((taps - 1, 0), (0, 0)))
    conv_sum = jnp.zeros((length, recurrent_branch_rows.shape[1]), jnp.float32)
    for tap_index in range(taps):
        conv_sum = conv_sum + padded[tap_index : tap_index + length] * convolution_kernel[
            tap_index
        ].astype(jnp.float32)
    conv_rows = conv_sum.astype(jnp.bfloat16)
    blocks = decay_gate_matrix.shape[0]
    blocked = conv_rows.reshape(length, blocks, -1)
    recurrence_gate = jax.nn.sigmoid(
        jnp.einsum(
            "tni,nij->tnj", blocked, decay_gate_matrix, preferred_element_type=jnp.float32
        ).reshape(length, -1)
    )
    input_rate = jax.nn.sigmoid(
        jnp.einsum(
            "tni,nij->tnj", blocked, input_gate_matrix, preferred_element_type=jnp.float32
        ).reshape(length, -1)
    )
    decay_log_values = (
        -8.0 * jax.nn.softplus(-base_decay_logit) * recurrence_gate + extra_log_decay[:, None]
    )
    decay = jnp.exp(decay_log_values)
    drive = (
        jnp.sqrt(-jnp.expm1(2.0 * decay_log_values)) * input_rate * conv_rows.astype(jnp.float32)
    )
    _, hidden = lax.associative_scan(combine, (decay, drive), axis=0)
    return (hidden * gate_branch_rows.astype(jnp.float32)).astype(jnp.bfloat16)


def per_device(
    tokens,
    recurrent_norm_gain,
    feedforward_norm_gain,
    gate_projection_weight,
    recurrent_projection_weight,
    convolution_kernel,
    decay_gate_matrix,
    input_gate_matrix,
    base_decay_logit,
    extra_log_decay,
    output_projection_weight,
    up_projection_weight,
    down_projection_weight,
):
    whole_rows = lax.all_gather(tokens, "tp", axis=1, tiled=True)
    normed = rms_rows(whole_rows, recurrent_norm_gain)
    columns = normed
    gate_pre = jnp.dot(
        columns,
        lax.all_gather(gate_projection_weight, "fs", axis=0, tiled=True),
        preferred_element_type=jnp.float32,
    )
    recur_pre = jnp.dot(
        columns,
        lax.all_gather(recurrent_projection_weight, "fs", axis=0, tiled=True),
        preferred_element_type=jnp.float32,
    )
    gate_branch_rows = jax.nn.gelu(gate_pre).astype(jnp.bfloat16)
    recurrent_branch_rows = recur_pre.astype(jnp.bfloat16)
    mixed_output = recurrent_state(
        recurrent_branch_rows,
        gate_branch_rows,
        convolution_kernel,
        decay_gate_matrix,
        input_gate_matrix,
        base_decay_logit,
        extra_log_decay,
    )
    partials = jnp.dot(
        mixed_output,
        lax.all_gather(output_projection_weight, "fs", axis=1, tiled=True),
        preferred_element_type=jnp.float32,
    )
    residual = (
        tokens.astype(jnp.float32)
        + lax.psum_scatter(
            partials.astype(jnp.bfloat16), "tp", scatter_dimension=1, tiled=True
        ).astype(jnp.float32)
    ).astype(jnp.bfloat16)
    middle = lax.all_gather(residual, "tp", axis=1, tiled=True)
    channel_in = rms_rows(middle, feedforward_norm_gain)
    columns = channel_in
    upward = jnp.dot(
        columns,
        lax.all_gather(up_projection_weight, "fs", axis=0, tiled=True),
        preferred_element_type=jnp.float32,
    )
    positive = jnp.maximum(upward, 0.0)
    squared = (positive * positive).astype(jnp.bfloat16)
    down_terms = jnp.dot(
        squared,
        lax.all_gather(down_projection_weight, "fs", axis=1, tiled=True),
        preferred_element_type=jnp.float32,
    )
    summed_down = lax.psum_scatter(
        down_terms.astype(jnp.bfloat16), "tp", scatter_dimension=1, tiled=True
    ).astype(jnp.float32)
    return (residual.astype(jnp.float32) + summed_down).astype(jnp.bfloat16)

PIECES, SPLIT = 2, 2
POOL = 40
UP, DOWN = (3, 4), (5, 6)
LIMIT = 58 * 2**20
TILE = 64


class Link:
    def __init__(self, pool):
        self.pool, self.started = pool, []

    def drain(self, moving, only):
        if only is None:
            moving.wait_send()
        else:
            pl.when(only)(moving.wait_send)

    def send(self, source, target, arrival, peer, only=None):
        turn = len(self.started)
        if turn >= POOL:
            self.drain(*self.started[turn - POOL])
        moving = pltpu.make_async_remote_copy(
            src_ref=source,
            dst_ref=target,
            send_sem=self.pool.at[turn % POOL],
            recv_sem=arrival,
            device_id=peer,
            device_id_type=MESH,
        )
        self.started.append((moving, only))
        if only is None:
            moving.start()
        else:
            pl.when(only)(moving.start)

    def finish(self):
        for moving, only in self.started[-POOL:]:
            self.drain(moving, only)


def arrive(target, arrival, peer):
    pltpu.make_async_remote_copy(
        src_ref=target,
        dst_ref=target,
        send_sem=arrival,
        recv_sem=arrival,
        device_id=peer,
        device_id_type=MESH,
    ).wait_recv()


class Where:
    def __init__(self):
        self.place, self.row = lax.axis_index("fs"), lax.axis_index("tp")
        self.plane = lax.axis_index("grp")
        place = self.place
        self.near = place + 1 - 2 * lax.rem(place, 2)
        self.mid = 3 - place
        self.inner = lax.rem((place + 1) // 2, 2)
        self.is_inner, self.is_outer = self.inner == 1, self.inner == 0
        far = place // 2
        self.order = [place, self.near, 2 - far, 3 - 3 * far]
        near, other = self.near, self.order[2]
        self.sooner = [place, near + self.inner * (other - near)]
        self.sooner += [other + self.inner * (near - other), self.order[3]]
        self.across, self.beside, self.corner = self.row ^ 2, self.row ^ 1, self.row ^ 3


def greet(at):
    barrier = pltpu.get_barrier_semaphore()
    peers = [{"fs": spot} for spot in at.order[1:]]
    peers += [{"tp": at.beside}, {"tp": at.across}, {"grp": 1 - at.plane}]
    for peer in peers:
        pl.semaphore_signal(barrier, inc=1, device_id=peer, device_id_type=MESH)
    pl.semaphore_wait(barrier, len(peers))


class Gather:
    def __init__(self, at, link, pair, own, held, arrived):
        self.at, self.link, self.own, self.held, self.arrived = at, link, own, held, arrived
        self.pair = pair
        self.step = own.shape[0] // PIECES

    def piece(self, origin, part, number):
        return self.held.at[origin, part, pl.ds(number * self.step, self.step)]

    def send(self, source, origin, part, number, peer, only=None):
        self.link.send(
            source,
            self.piece(origin, part, number),
            self.arrived.at[origin, part, number],
            peer,
            only,
        )

    def wait(self, origin, part, number):
        arrive(
            self.piece(origin, part, number),
            self.arrived.at[origin, part, number],
            {"tp": self.at.beside},
        )

    def begin(self, along=True, aside=True):
        at = self.at
        for number in range(PIECES):
            source = self.own.at[pl.ds(number * self.step, self.step)]
            if along:
                self.send(source, at.place, at.row, number, {"fs": at.near})
                if not self.pair:
                    self.send(source, at.place, at.row, number, {"fs": at.mid}, at.is_inner)
            if aside:
                self.send(source, at.place, at.row, number, {"tp": at.across})
                self.send(source, at.place, at.row, number, {"tp": at.beside})

    def relay(self, k):
        at, origin = self.at, self.at.order[k]
        for number in range(PIECES):
            self.wait(origin, at.row, number)
            source = self.piece(origin, at.row, number)
            onward = {"fs": at.mid if k == 1 else at.near}
            if not self.pair:
                self.send(source, origin, at.row, number, onward, at.is_inner)
            self.send(source, origin, at.row, number, {"tp": at.across})
            self.send(source, origin, at.row, number, {"tp": at.beside})

    def cross(self, k):
        at, origin = self.at, self.at.order[k]
        for number in range(PIECES):
            self.wait(origin, at.across, number)
            source = self.piece(origin, at.across, number)
            self.send(source, origin, at.across, number, {"tp": at.beside})

    def normalise(self, k, norm_gain, target):
        at, origin = self.at, self.at.order[k]
        for number in range(PIECES):
            self.wait(origin, at.beside, number)
            self.wait(origin, at.corner, number)
        length, width = self.own.shape
        parts_of = self.held.shape[1]

        def tile(index, carry):
            rows = pl.ds(pl.multiple_of(index * TILE, TILE), TILE)
            parts = [self.held[origin, p, rows].astype(jnp.float32) for p in range(parts_of)]
            total = sum(jnp.sum(part * part, axis=-1, keepdims=True) for part in parts)
            inverse = lax.rsqrt(total / (parts_of * width) + 1e-06)
            for number, part in enumerate(parts):
                columns = pl.ds(number * width, width)
                target[rows, columns] = (part * inverse * norm_gain[:, columns]).astype(
                    target.dtype
                )
            return carry

        lax.fori_loop(0, length // TILE, tile, 0)


class Scatter:
    def __init__(self, at, link, pair, terms, from_core, to_x, from_x, to_z, from_z, sems):
        self.pair = pair
        self.at, self.link, self.terms = at, link, terms
        self.from_core, self.to_x, self.from_x = from_core, to_x, from_x
        self.to_z, self.from_z = to_z, from_z
        self.core_sems, self.x_sems, self.z_sems = sems
        self.step = terms.shape[2] // SPLIT

    def rows(self, number):
        return pl.ds(number * self.step, self.step)

    def core(self, k):
        at = self.at
        for side, part in ((1, at.corner), (0, at.beside)):
            self.link.send(
                self.terms.at[k, part],
                self.from_core.at[side, k],
                self.core_sems.at[side, k],
                {"tp": at.beside},
            )

    def x(self, k):
        at = self.at
        arrive(self.from_core.at[1, k], self.core_sems.at[1, k], {"tp": at.beside})
        for number in range(SPLIT):
            rows = self.rows(number)
            mine = self.terms[k, at.across, rows].astype(jnp.float32)
            theirs = self.from_core[1, k, rows].astype(jnp.float32)
            self.to_x[k, rows] = (mine + theirs).astype(self.to_x.dtype)
            self.link.send(
                self.to_x.at[k, rows],
                self.from_x.at[k, rows],
                self.x_sems.at[k, number],
                {"tp": at.across},
            )

    def joined(self, k, number):
        rows = self.rows(number)
        mine = self.terms[k, self.at.row, rows].astype(jnp.float32)
        mine = mine + self.from_core[0, k, rows].astype(jnp.float32)
        return mine + self.from_x[k, rows].astype(jnp.float32)

    def taken(self, slot, number):
        rows = self.rows(number)
        arrive(
            self.from_z.at[slot, rows], self.z_sems.at[slot, number], {"fs": self.at.near}
        )
        return self.from_z[slot, rows].astype(jnp.float32)

    def ready(self, k, number):
        at, rows = self.at, self.rows(number)
        if not number:
            arrive(self.from_core.at[0, k], self.core_sems.at[0, k], {"tp": at.beside})
        arrive(self.from_x.at[k, rows], self.x_sems.at[k, number], {"tp": at.across})

    def z(self, k):
        at = self.at
        comes = {2: 0, 3: 1, 1: 4}[k]
        if self.pair:
            for number in range(SPLIT):
                rows = self.rows(number)
                self.ready(k, number)
                self.to_z[k, rows] = self.joined(k, number).astype(self.to_z.dtype)
                self.link.send(
                    self.to_z.at[k, rows],
                    self.from_z.at[2, rows],
                    self.z_sems.at[2, number],
                    {"fs": at.near},
                )
            return
        peer = at.near if k == 1 else at.near + at.inner * (at.mid - at.near)
        slot = {2: 3 * at.inner, 3: 1 + 3 * at.inner, 1: 2}[k]
        for number in range(SPLIT):
            rows = self.rows(number)
            self.ready(k, number)

            @pl.when(at.is_inner)
            def _():
                total = self.joined(k, number) + self.taken(comes, number)
                self.to_z[k, rows] = total.astype(self.to_z.dtype)

            @pl.when(at.is_outer)
            def _():
                self.to_z[k, rows] = self.joined(k, number).astype(self.to_z.dtype)

            self.link.send(
                self.to_z.at[k, rows],
                self.from_z.at[slot, rows],
                self.z_sems.at[slot, number],
                {"fs": peer},
            )

    def own(self, base, target):
        at = self.at
        for number in range(SPLIT):
            rows = self.rows(number)
            self.ready(0, number)
            if self.pair:
                total = self.joined(0, number) + self.taken(2, number)
                target[rows] = (base[rows].astype(jnp.float32) + total).astype(target.dtype)
                continue

            @pl.when(at.is_inner)
            def _():
                total = self.joined(0, number) + self.taken(2, number) + self.taken(3, number)
                target[rows] = (base[rows].astype(jnp.float32) + total).astype(target.dtype)

            @pl.when(at.is_outer)
            def _():
                total = self.joined(0, number) + self.taken(2, number)
                target[rows] = (base[rows].astype(jnp.float32) + total).astype(target.dtype)


class Weights:
    def __init__(self, at, link, chunks, moves):
        self.at, self.link, self.chunks, self.moves = at, link, chunks, moves

    def spread(self, number, k, only):
        at, (leaving, landing, extra) = self.at, self.chunks[number]
        owner = at.order[k]
        if extra:
            if k == 3 or k == 1 and only is at.is_inner:
                return
            only = at.is_outer if k == 1 else only
        self.link.send(
            leaving(owner, at.plane),
            landing(at.place, at.plane),
            self.moves.at[number, 0, at.place],
            {"fs": owner},
            only,
        )

    def forward(self, number, k, only):
        at, (_, landing, extra) = self.at, self.chunks[number]
        source, peer = at.sooner[k], {"grp": 1 - at.plane}
        here = landing(source, at.plane)

        def arrived():
            arrive(here, self.moves.at[number, 0, source], peer)

        if extra and only is at.is_outer:
            return
        only = at.is_inner if extra else only
        if only is None:
            arrived()
        else:
            pl.when(only)(arrived)
        self.link.send(here, here, self.moves.at[number, 1, source], peer, only)

    def wait(self, number):
        at, (_, landing, extra) = self.at, self.chunks[number]

        def arrived():
            for source in at.order[1:]:
                arrive(
                    landing(source, 1 - at.plane),
                    self.moves.at[number, 1, source],
                    {"grp": 1 - at.plane},
                )

        if extra:
            pl.when(at.is_inner)(arrived)
        else:
            arrived()


def recurrence(both, taps, decay_map, input_map, rate, extra):
    wide = jnp.float32
    size = both.shape[1] // 2
    block = decay_map[0].shape[1]
    recur = both[:, size:].astype(jnp.bfloat16).astype(wide)
    length = recur.shape[0]
    position = lax.broadcasted_iota(jnp.int32, recur.shape, 0)
    count = taps.shape[0]
    conv = recur * taps[count - 1 : count].astype(wide)
    for tap in range(count - 1):
        back = count - 1 - tap
        earlier = jnp.where(position >= back, pltpu.roll(recur, back, 0), 0.0)
        conv = conv + earlier * taps[tap : tap + 1].astype(wide)
    conv_rows = conv.astype(jnp.bfloat16)

    def mapped(matrix):
        products = [
            jnp.dot(
                conv_rows[:, n * block : (n + 1) * block], matrix[n], preferred_element_type=wide
            )
            for n in range(size // block)
        ]
        return jax.nn.sigmoid(jnp.concatenate(products, axis=1))

    recur_gate, input_rate = mapped(decay_map), mapped(input_map)
    log_decay = rate * recur_gate + extra
    decay = jnp.exp(log_decay)
    spread = -jnp.tanh(log_decay) * (decay * decay + 1.0)
    drive = jnp.sqrt(spread) * input_rate * conv_rows.astype(wide)
    back = 1
    while back < length:
        inside = position >= back
        drive = drive + decay * jnp.where(inside, pltpu.roll(drive, back, 0), 0.0)
        if back * 2 < length:
            decay = decay * jnp.where(inside, pltpu.roll(decay, back, 0), 1.0)
        back *= 2
    gate_rows = jax.nn.gelu(both[:, :size]).astype(jnp.bfloat16)
    return (drive * gate_rows.astype(wide)).astype(jnp.bfloat16)


def layer_kernel(
    tokens_from, gain_one_from, gain_two_from, taps_from, decay_map_from, input_map_from,
    logit_from, extra_from, gate, recur, outward, upward, downward, out,
    held_one, held_two, residual, normed, mixed, squared, both_w, out_w, up_w, down_w, extra,
    terms, from_core, to_x, from_x, to_z, from_z,
    tokens, gain_one, gain_two, taps, decay_map, input_map, logit, extra_own,
    small_sems, pool, arrived, core_sems, x_sems, z_sems, moves, extra_sems, local_sems,
):
    at = Where()
    small = []
    for number, (source, target) in enumerate(
        (
            (tokens_from, tokens), (extra_from, extra_own), (gain_one_from, gain_one),
            (taps_from, taps), (decay_map_from, decay_map), (input_map_from, input_map),
            (logit_from, logit), (gain_two_from, gain_two),
        )
    ):
        small.append(pltpu.make_async_copy(source, target, small_sems.at[number]))
        small[-1].start()
    greet(at)
    for moving in small:
        moving.wait()
    link = Link(pool)
    length, width = tokens.shape
    depth, size = gate.shape[0], taps.shape[1] // 2
    most = up_w.shape[1]
    least = upward.shape[1] // 2 - most
    half, place = depth // 2, at.place

    def spot(start, count, step):
        return pl.ds(pl.multiple_of(start, step), count)

    def by_rows(weight, joined, columns, first, begins, extra=False):
        def leaving(owner, plane):
            return weight.at[spot(plane * half, half, half), spot(begins(owner), columns, 128)]

        def landing(source, plane):
            rows = spot(source * depth + plane * half, half, half)
            return joined.at[rows, pl.ds(first, columns)]

        return leaving, landing, extra

    def by_columns(weight, joined, rows_of, first, begins, extra=False):
        share = rows_of // 2

        def leaving(owner, plane):
            return weight.at[spot(begins(owner) + plane * share, share, 64)]

        def landing(source, plane):
            rows = spot(first + plane * share, share, 64)
            return joined.at[rows, spot(source * width, width, width)]

        return leaving, landing, extra

    def of_pair(owner):
        return lax.rem(owner, 2) * size

    def basic(owner):
        return owner * least + (owner + 1) // 3 * (most - least) + owner // 3 * (most - least)

    def further(owner):
        return basic(owner) + least

    chunks = [
        by_rows(gate, both_w, size, 0, of_pair),
        by_rows(recur, both_w, size, size, of_pair),
        by_columns(outward, out_w, size, 0, of_pair),
        by_rows(upward, up_w, least, 0, basic),
        by_rows(upward, up_w, most - least, least, further, True),
        by_columns(downward, down_w, least, 0, basic),
        by_columns(downward, down_w, most - least, least, further, True),
    ]
    weights = Weights(at, link, chunks, moves)

    def spread(numbers, ks=(1, 2, 3), only=None):
        for k in ks:
            for number in numbers:
                weights.spread(number, k, only)

    def forward(numbers, ks=(1, 2, 3), only=None):
        for k in ks:
            for number in numbers:
                weights.forward(number, k, only)

    first = Gather(at, link, True, tokens, held_one, arrived)
    spread((0, 1), (1,))
    first.begin()
    spread((0, 1), (2, 3))
    link.send(extra_own.at[0], extra.at[place], extra_sems.at[place], {"fs": at.near})
    extra[place] = extra_own[0]
    local = []
    for number, (leaving, landing, extra_part) in enumerate(chunks):
        for plane in range(2):
            moving = pltpu.make_async_copy(
                leaving(place, plane), landing(place, plane), local_sems.at[number, plane]
            )
            local.append((moving, extra_part))
            if extra_part:
                pl.when(at.is_inner)(moving.start)
            else:
                moving.start()
    held_one[place, at.row] = tokens[...]
    first.cross(0)
    first.normalise(0, gain_one, normed.at[0])
    forward((0, 1), (1,))
    first.relay(1)
    forward((0, 1), (2,))
    first.cross(1)
    spread((2,))
    first.normalise(1, gain_one, normed.at[1])
    arrive(extra.at[at.near], extra_sems.at[at.near], {"fs": at.near})
    for moving, extra_part in local:
        if extra_part:
            pl.when(at.is_inner)(moving.wait)
        else:
            moving.wait()
    forward((0, 1), (3,))
    forward((2,), (1,))
    for number in range(2):
        weights.wait(number)
    spread(UP)
    side = lax.rem(place, 2)
    blocks = size // decay_map.shape[1]
    own_taps = taps[:, spot(side * size, size, size)]
    own_logit = logit[:, spot(side * size, size, size)]
    rate = -8.0 * (
        jnp.maximum(-own_logit, 0.0) + jnp.log1p(jnp.exp(-jnp.abs(own_logit)))
    )

    def mix(k):
        both = jnp.dot(normed[k], both_w[...], preferred_element_type=jnp.float32)
        added = jnp.transpose(jnp.broadcast_to(extra[at.order[k]], (size, length)))
        maps = [
            [matrix[side * blocks + n] for n in range(blocks)] for matrix in (decay_map, input_map)
        ]
        mixed[k] = recurrence(both, own_taps, *maps, rate, added)

    def project(k):
        for part in range(4):
            terms[0, k, part] = jnp.dot(
                mixed[k], out_w[:, pl.ds(part * width, width)], preferred_element_type=jnp.float32
            ).astype(terms.dtype)

    def scatter(turn):
        return Scatter(
            at, link, not turn, terms.at[turn], from_core.at[turn], to_x.at[turn], from_x.at[turn],
            to_z.at[turn], from_z.at[turn],
            (core_sems, x_sems, z_sems),
        )

    def raised(k, columns):
        product = jnp.dot(normed[k], up_w[:, columns], preferred_element_type=jnp.float32)
        positive = jnp.maximum(product, 0.0)
        squared[k, :, columns] = (positive * positive).astype(squared.dtype)

    def lift(k):
        raised(k, pl.ds(0, least))

        @pl.when(at.is_inner)
        def _():
            raised(k, pl.ds(least, most - least))

    summed = scatter(0)
    mix(1)
    forward((2,), (2,))
    mix(0)
    forward((2,), (3,))
    weights.wait(2)
    project(1)
    summed.core(1)
    project(0)
    summed.core(0)
    summed.x(1)
    summed.x(0)
    summed.z(1)
    spread(DOWN[:1], (2, 3, 1), at.is_inner)
    spread(DOWN[:1], (1,), at.is_outer)
    forward(UP[:1], (1,))
    summed.own(tokens, residual)

    second = Gather(at, link, False, residual, held_two, arrived)
    second.begin()
    spread(DOWN[1:], (1,), at.is_outer)
    held_two[place, at.row] = residual[...]
    forward(UP[:1], (2, 3))
    forward(UP[1:])
    forward(DOWN[:1], (1,))
    second.relay(1)
    spread(DOWN[:1], (2, 3), at.is_outer)
    spread(DOWN[1:], (2,), at.is_outer)
    second.cross(0)
    second.relay(2)
    spread(DOWN[1:], (2,), at.is_inner)
    second.cross(1)
    forward(DOWN[:1], (2,))
    second.normalise(0, gain_two, normed.at[0])
    for number in UP:
        weights.wait(number)
    lift(0)
    second.normalise(1, gain_two, normed.at[1])
    lift(1)
    second.relay(3)
    second.cross(2)
    forward(DOWN[:1], (3,))
    forward(DOWN[1:], (2,))
    second.normalise(2, gain_two, normed.at[2])
    lift(2)
    second.cross(3)
    forward(DOWN[1:], (1,))
    second.normalise(3, gain_two, normed.at[3])
    forward(DOWN[1:], (3,))
    def lowered(k, count):
        for part in range(4):
            terms[1, k, part] = jnp.dot(
                squared[k, :, pl.ds(0, count)],
                down_w[pl.ds(0, count), pl.ds(part * width, width)],
                preferred_element_type=jnp.float32,
            ).astype(terms.dtype)

    def lower(k):
        @pl.when(at.is_inner)
        def _():
            lowered(k, most)

        @pl.when(at.is_outer)
        def _():
            lowered(k, least)

    last = scatter(1)
    lift(3)
    for number in DOWN:
        weights.wait(number)
    lower(3)
    last.core(3)
    lower(2)
    last.core(2)
    last.x(3)
    lower(1)
    last.core(1)
    last.x(2)
    lower(0)
    last.core(0)
    last.x(1)
    last.x(0)
    last.z(3)
    last.z(2)
    last.z(1)
    last.own(residual, out)
    link.finish()


def per_device_owned(
    tokens,
    recurrent_norm_gain,
    feedforward_norm_gain,
    gate_projection_weight,
    recurrent_projection_weight,
    convolution_kernel,
    decay_gate_matrix,
    input_gate_matrix,
    base_decay_logit,
    extra_log_decay,
    output_projection_weight,
    up_projection_weight,
    down_projection_weight,
):
    length, width = tokens.shape
    depth, size = gate_projection_weight.shape[0], gate_projection_weight.shape[1] // 2
    hidden = up_projection_weight.shape[1] // 4
    hidden += hidden // 4
    kind, wide = tokens.dtype, jnp.float32
    vmem, anywhere = pl.BlockSpec(memory_space=pltpu.VMEM), pl.BlockSpec(memory_space=pltpu.HBM)
    dma, block = pltpu.SemaphoreType.DMA, (length, width)
    scratch = [
        ((4, 4) + block, kind),
        ((4, 4) + block, kind),
        (block, kind),
        ((4, length, 4 * width), kind),
        ((4, length, size), kind),
        ((4, length, hidden), kind),
        ((4 * depth, 2 * size), kind),
        ((size, 4 * width), kind),
        ((4 * depth, hidden), kind),
        ((hidden, 4 * width), kind),
        ((4, 1, length), wide),
        ((2, 4, 4) + block, kind),
        ((2, 2, 4) + block, kind),
        ((2, 4) + block, kind),
        ((2, 4) + block, kind),
        ((2, 4) + block, kind),
        ((2, 5) + block, kind),
        (block, kind),
        ((1, 4 * width), wide),
        ((1, 4 * width), wide),
        (convolution_kernel.shape, convolution_kernel.dtype),
        (decay_gate_matrix.shape, decay_gate_matrix.dtype),
        (input_gate_matrix.shape, input_gate_matrix.dtype),
        ((1, base_decay_logit.shape[0]), wide),
        ((1, 1, length), wide),
    ]
    return pl.pallas_call(
        layer_kernel,
        out_shape=jax.ShapeDtypeStruct(block, kind),
        in_specs=[anywhere] * 13,
        out_specs=vmem,
        scratch_shapes=[pltpu.VMEM(*entry) for entry in scratch]
        + [
            dma((8,)),
            dma((POOL,)),
            dma((4, 4, PIECES)),
            dma((2, 4)),
            dma((4, SPLIT)),
            dma((5, SPLIT)),
            dma((7, 2, 4)),
            dma((4,)),
            dma((7, 2)),
        ],
        compiler_params=pltpu.CompilerParams(
            collective_id=1, has_side_effects=True, vmem_limit_bytes=LIMIT
        ),
    )(
        tokens,
        recurrent_norm_gain.reshape(1, -1),
        feedforward_norm_gain.reshape(1, -1),
        convolution_kernel,
        decay_gate_matrix,
        input_gate_matrix,
        base_decay_logit.reshape(1, -1),
        extra_log_decay.reshape(1, 1, -1),
        gate_projection_weight,
        recurrent_projection_weight,
        output_projection_weight,
        up_projection_weight,
        down_projection_weight,
    )


def solution(mesh):
    placed = (
        P(("grp", "fs"), "tp"),
        P(),
        P(),
        P("fs", "tp"),
        P("fs", "tp"),
        P(None, "tp"),
        P("tp", None, None),
        P("tp", None, None),
        P("tp"),
        P(("grp", "fs")),
        P("tp", "fs"),
        P("fs", "tp"),
        P("tp", "fs"),
    )
    owners = mesh.shape["fs"] * mesh.shape["tp"]
    fitting = mesh.shape["tp"] == 4 and mesh.shape["grp"] == 2 and mesh.shape["fs"] == 4

    def run(*arrays):
        owned = fitting and arrays[6].shape[0] == owners
        body = per_device_owned if owned else per_device
        return jax.shard_map(
            body, mesh=mesh, in_specs=placed, out_specs=P(("grp", "fs"), "tp"), check_vma=False
        )(*arrays)

    return run
```
